256 devices in a mesh: ep: 16 (over y, x), tp: 16 (over z, core).
Axes of the slice: x: 4, y: 4, z: 8, core: 2. Of those that a mesh axis runs over, the one named last changes fastest.
Arguments:
- hidden: bfloat16 [640, 4096], P('ep', 'tp'), may hold values from -6 to 6
- positions: int32 [640], P('ep'), may hold values from 0 to 16383
- ret_state: float32 [640, 16, 128, 128], P('ep', 'tp'), may hold values from -1.5 to 1.5
- query_weight: bfloat16 [4096, 2048], P('ep', 'tp'), may hold values from -0.09375 to 0.09375
- key_weight: bfloat16 [4096, 2048], P('ep', 'tp'), may hold values from -0.09375 to 0.09375
- value_weight: bfloat16 [4096, 2048], P('ep', 'tp'), may hold values from -0.09375 to 0.09375
- gate_weight: bfloat16 [4096, 2048], P('ep', 'tp'), may hold values from -0.09375 to 0.09375
- head_gain: float32 [2048], P('tp'), may hold values from 0.1 to 1.9
- out_weight: bfloat16 [2048, 4096], P(None, 'tp'), may hold values from -0.125 to 0.125
- mix_gain: float32 [4096], replicated, may hold values from 0.1 to 1.9
- ffn_gain: float32 [4096], replicated, may hold values from 0.1 to 1.9
- expert_gate: bfloat16 [32, 4096, 2048], P('ep', None, 'tp'), may hold values from -0.09375 to 0.09375
- expert_up: bfloat16 [32, 4096, 2048], P('ep', None, 'tp'), may hold values from -0.09375 to 0.09375
- expert_down: bfloat16 [32, 2048, 4096], P('ep', None, 'tp'), may hold values from -0.125 to 0.125
- route_ids: int32 [640, 2], P('ep'), may hold values from 0 to 31, as said below
- route_weight: float32 [640, 2], P('ep'), may hold values from 0.25 to 1
Outputs:
- updated: bfloat16 [640, 4096], P('ep', 'tp')
- next_state: float32 [640, 16, 128, 128], P('ep', 'tp')
The draws below stay inside these ranges and needn't reach their ends.
Inputs may be any that keep to these rules, and one draw needn't show every extreme that they name: `route_ids`: each row names two different experts of one group, the group being the numbers g * 8 to g * 8 + 7; in the rows of one device (aligned blocks of 40 rows) no expert is named more than 4 times, and some expert is named exactly 4 times.
All inputs are finite; a program needn't handle non-finite values.
Results may differ from the reference program's by a relative error of at most 0.014.
Values may be sent and summed in bfloat16 or wider, within the bound.
A program may use at most 64 MiB of HBM per device.

```python
import jax
import jax.numpy as jnp
from jax import lax

D = 4096
HEADS = 16
HEAD = 128
RD = 2048
FF = 2048
GROUPS = 4
EXPERTS = 32
TOP = 2
B_DEV = 40
BATCH = 640
CAP = 4
MAXPOS = 16384
N_EP = 16


def draw_route_ids(key, part):
    blocks = BATCH // B_DEV
    group_size = EXPERTS // GROUPS
    order_key, shift_key = jax.random.split(key)
    orders = jax.vmap(lambda item: jax.random.permutation(item, B_DEV))(jax.random.split(order_key, blocks))
    shifts = jax.random.randint(shift_key, (blocks, GROUPS), 0, group_size)
    group = orders % GROUPS
    within = orders // GROUPS
    offset = jnp.take_along_axis(shifts, group, axis=1)
    first = (within + offset) % group_size
    second = (first + 1) % group_size
    pairs = jnp.stack([group * group_size + first, group * group_size + second], axis=-1)
    return pairs.reshape(BATCH, TOP).astype(jnp.int32)


def place_ends(values, key, least, largest):
    spot = [jax.random.randint(jax.random.fold_in(key, axis), (), 0, length) for axis, length in enumerate(values.shape)]
    longest = values.shape.index(max(values.shape))
    beside = spot[:longest] + [(spot[longest] + 1) % values.shape[longest]] + spot[longest + 1:]
    return values.at[tuple(spot)].set(least).at[tuple(beside)].set(largest)


def block_levels(own_key, extent, shards, low, largest):
    def one(axis_at, blocks):
        draws = jax.random.uniform(jax.random.fold_in(jax.random.fold_in(own_key, 6), axis_at), (blocks,), jnp.float32, low / len(shards), largest / len(shards))
        return jnp.repeat(jnp.exp(draws), extent[axis_at] // blocks).reshape((-1,) + (1,) * (len(extent) - axis_at - 1))

    level = one(*shards[0])
    for cut in shards[1:]:
        level = level * one(*cut)
    return level


def scatter_about(rng, dims, scale, bound, cuts=(), held_as=jnp.bfloat16):
    values = scale * jax.random.normal(rng, dims, jnp.float32)
    if cuts:
        values = values * block_levels(rng, dims, cuts, -0.22, 0.18)
    return jnp.clip(values, -bound, bound).astype(held_as)


def setup_inputs(seed: int = 0) -> dict:
    keys = jax.random.split(jax.random.key(seed), 17)
    hidden = scatter_about(keys[0], (BATCH, D), 1.0, 6.0, ((0, 16), (1, 16)))
    positions = place_ends(jax.random.randint(keys[1], (BATCH,), 0, MAXPOS), jax.random.fold_in(keys[1], 1), 0, MAXPOS - 1).astype(jnp.int32)
    ret_state = scatter_about(keys[2], (BATCH, HEADS, HEAD, HEAD), 0.25, 1.5, ((0, 16), (1, 16)), jnp.float32)
    query_weight = scatter_about(keys[3], (D, RD), D ** -0.5, 0.09375, ((0, 16), (1, 16)))
    key_weight = scatter_about(keys[4], (D, RD), D ** -0.5, 0.09375, ((0, 16), (1, 16)))
    value_weight = scatter_about(keys[5], (D, RD), D ** -0.5, 0.09375, ((0, 16), (1, 16)))
    gate_weight = scatter_about(keys[6], (D, RD), D ** -0.5, 0.09375, ((0, 16), (1, 16)))
    head_gain = jnp.clip(1.0 + 0.18 * jax.random.normal(keys[7], (RD,), jnp.float32), 0.1, 1.9)
    out_weight = scatter_about(keys[8], (RD, D), RD ** -0.5, 0.125, ((1, 16),))
    mix_gain = jnp.clip(1.0 + 0.18 * jax.random.normal(keys[9], (D,), jnp.float32), 0.1, 1.9)
    ffn_gain = jnp.clip(1.0 + 0.18 * jax.random.normal(keys[10], (D,), jnp.float32), 0.1, 1.9)
    expert_gate = scatter_about(keys[11], (EXPERTS, D, FF), D ** -0.5, 0.09375, ((0, 16), (2, 16)))
    expert_up = scatter_about(keys[12], (EXPERTS, D, FF), D ** -0.5, 0.09375, ((0, 16), (2, 16)))
    expert_down = scatter_about(keys[13], (EXPERTS, FF, D), FF ** -0.5, 0.125, ((0, 16), (2, 16)))
    route_ids = draw_route_ids(jax.random.fold_in(keys[16], 71), 0)
    route_weight = jnp.clip(0.25 + 0.75 * jax.random.uniform(keys[15], (BATCH, TOP), jnp.float32) ** block_levels(keys[15], (BATCH, TOP), ((0, 16),), -0.2, 0.2), 0.25, 1.0)
    return dict(hidden=hidden, positions=positions, ret_state=ret_state, query_weight=query_weight, key_weight=key_weight, value_weight=value_weight, gate_weight=gate_weight, head_gain=head_gain, out_weight=out_weight, mix_gain=mix_gain, ffn_gain=ffn_gain, expert_gate=expert_gate, expert_up=expert_up, expert_down=expert_down, route_ids=route_ids, route_weight=route_weight)


epsilon = 1e-06
rope_base = 10000.0

def rms_scale(rows, gain):
    values = rows.astype(jnp.float32)
    factor = lax.rsqrt(lax.optimization_barrier(jnp.mean(values * values, axis=-1, keepdims=True)) + epsilon)
    return (values * factor * gain).astype(jnp.bfloat16)

def log_decay(head_ids):
    return jnp.log(1.0 - 2.0 ** (-5.0 - 5.0 * head_ids.astype(jnp.float32) / (HEADS - 1)))

def rotate(values, positions):
    width = values.shape[-1]
    inverse = 1.0 / rope_base ** (jnp.arange(0, width, 2, dtype=jnp.float32) / width)
    angle = positions.astype(jnp.float32)[:, None, None] * inverse[None, None, :]
    cosine = jnp.cos(angle)
    sine = jnp.sin(angle)
    first = values[..., :width // 2]
    second = values[..., width // 2:]
    return jnp.concatenate([first * cosine - second * sine, first * sine + second * cosine], axis=-1)

def retain(query, key_rows, value_rows, gate_rows, ret_state, positions, head_ids, head_gain):
    batch = query.shape[0]
    heads = head_ids.shape[0]

    def split(array):
        return array.astype(jnp.float32).reshape(batch, heads, HEAD)
    rotated_query = rotate(split(query), positions)
    rotated_key = rotate(split(key_rows), positions) * HEAD ** (-0.5)
    value_heads = split(value_rows)
    decay = jnp.exp(log_decay(head_ids))
    next_state = decay[None, :, None, None] * ret_state + rotated_key[..., :, None] * value_heads[..., None, :]
    read = jnp.einsum('bhd,bhde->bhe', rotated_query, next_state, precision=lax.Precision.HIGHEST)
    centered = read - lax.optimization_barrier(jnp.mean(read, axis=-1, keepdims=True))
    normal = centered * lax.rsqrt(lax.optimization_barrier(jnp.mean(centered * centered, axis=-1, keepdims=True)) + epsilon)
    mixed = normal.reshape(batch, heads * HEAD) * head_gain * jax.nn.silu(gate_rows.astype(jnp.float32))
    return (mixed.astype(jnp.bfloat16), next_state)

def reference(hidden, positions, ret_state, query_weight, key_weight, value_weight, gate_weight, head_gain, out_weight, mix_gain, ffn_gain, expert_gate, expert_up, expert_down, route_ids, route_weight):
    normed = rms_scale(hidden, mix_gain)

    def project(weight):
        return jnp.dot(normed, weight, preferred_element_type=jnp.float32).astype(jnp.bfloat16)
    mixed, next_state = retain(project(query_weight), project(key_weight), project(value_weight), project(gate_weight), ret_state, positions, jnp.arange(HEADS, dtype=jnp.int32), head_gain)
    after = (hidden.astype(jnp.float32) + jnp.dot(mixed, out_weight, preferred_element_type=jnp.float32)).astype(jnp.bfloat16)
    inner = rms_scale(after, ffn_gain)
    pair_count = BATCH * TOP
    chosen = route_ids.reshape(pair_count).astype(jnp.int32)
    pair_rows = jnp.repeat(inner, TOP, axis=0)
    onehot = (chosen[:, None] == jnp.arange(EXPERTS, dtype=jnp.int32)[None, :]).astype(jnp.int32)
    ranks = lax.optimization_barrier(jnp.sum((jnp.cumsum(onehot, axis=0).astype(jnp.int32) - 1) * onehot, axis=1)).astype(jnp.int32)
    slots = jnp.arange(N_EP * CAP, dtype=jnp.int32)

    def one_expert(carry, index):
        select = ((chosen[None, :] == index) & (ranks[None, :] == slots[:, None])).astype(jnp.bfloat16)
        rows = jnp.dot(select, pair_rows, preferred_element_type=jnp.float32).astype(jnp.bfloat16)
        gate = jnp.dot(rows, expert_gate[index], preferred_element_type=jnp.float32)
        lifted = jnp.dot(rows, expert_up[index], preferred_element_type=jnp.float32)
        activated = (jax.nn.silu(gate) * lifted).astype(jnp.bfloat16)
        result = jnp.dot(activated, expert_down[index], preferred_element_type=jnp.float32).astype(jnp.bfloat16)
        return (carry + jnp.dot(select.T, result, preferred_element_type=jnp.float32), None)
    pair_out, unused = lax.scan(one_expert, jnp.zeros((pair_count, D), jnp.float32), jnp.arange(EXPERTS, dtype=jnp.int32))
    weighted = lax.optimization_barrier(jnp.sum(pair_out.reshape(BATCH, TOP, D) * route_weight[:, :, None], axis=1))
    updated = (after.astype(jnp.float32) + weighted).astype(jnp.bfloat16)
    return (updated, next_state)
```

```python
import functools

import jax
import jax.numpy as jnp
import numpy as np
from jax import lax
from jax.experimental import pallas as pl
from jax.experimental.pallas import tpu as pltpu
from jax.sharding import PartitionSpec as P

MESH = pl.DeviceIdType.MESH
F32 = jnp.float32
BF16 = jnp.bfloat16
D = 4096
RD = 2048
HEADS = 16
HEAD = 128
ROWS = 40
COLS = 256
NEP = 16
NTP = 16
NZ = 8
SLOTS = 128
EPS = 1e-06


def constants():
    table = np.zeros((24, 128), np.float64)
    heads = np.arange(HEADS, dtype=np.float64)
    table[:HEADS] = (1.0 - 2.0 ** (-5.0 - 5.0 * heads / (HEADS - 1)))[:, None]
    inverse = 10000.0 ** (-np.arange(0, HEAD, 2, dtype=np.float64) / HEAD)
    table[HEADS] = np.concatenate([inverse, inverse])
    return table.astype(np.float32)


def ring_offset(i):
    half = i // 2 + 1
    return half + (i % 2) * (NZ - 2 * half)


def body(
    hidden,
    positions,
    ret_state,
    query_weight,
    key_weight,
    value_weight,
    gate_weight,
    head_gain,
    out_weight,
    mix_gain,
    ffn_gain,
    expert_gate,
    expert_up,
    expert_down,
    route_ids,
    route_weight,
    table,
    updated,
    next_state,
    v_hidden,
    v_pos,
    v_state,
    v_qkvg,
    v_head_gain,
    v_out,
    v_mix_gain,
    v_ffn_gain,
    v_gu,
    v_down,
    v_ids,
    v_weight,
    v_table,
    agbuf,
    xbuf,
    bsend,
    brecv,
    ssout,
    ssin,
    readbuf,
    cbuf,
    psend,
    dbuf,
    acc_gu,
    ebuf,
    acc_down,
    fsend,
    frecv,
    local_sem,
    a1_send,
    a1_recv,
    a2_send,
    a2_recv,
    ss_sem,
    b_send,
    b_recv,
    c_send,
    c_fwd,
    c_recv,
    d1_send,
    d1_recv,
    d_send,
    d_fwd,
    d_recv,
    e_send,
    e_fwd,
    e_recv,
    f_send,
    f_recv,
):
    ep = lax.axis_index("ep")
    tp = lax.axis_index("tp")
    z = tp // 2
    core = tp % 2
    other = 2 * z + 1 - core

    loads = [
        (hidden, v_hidden),
        (positions, v_pos),
        (table, v_table),
        (route_ids, v_ids),
        (route_weight, v_weight),
        (head_gain, v_head_gain),
        (mix_gain, v_mix_gain),
        (ffn_gain, v_ffn_gain),
        (query_weight, v_qkvg.at[:, pl.ds(0, 128)]),
        (key_weight, v_qkvg.at[:, pl.ds(128, 128)]),
        (value_weight, v_qkvg.at[:, pl.ds(256, 128)]),
        (gate_weight, v_qkvg.at[:, pl.ds(384, 128)]),
        (ret_state, v_state),
        (out_weight, v_out),
        (expert_gate, v_gu.at[:, :, pl.ds(0, 128)]),
        (expert_up, v_gu.at[:, :, pl.ds(128, 128)]),
        (expert_down, v_down),
    ]
    copies = [pltpu.make_async_copy(src, dst, local_sem.at[i]) for i, (src, dst) in enumerate(loads)]
    for copy in copies[:12]:
        copy.start()

    barrier = pltpu.get_barrier_semaphore()

    def greet_plane(i, carry):
        peer = (ep + i) % NEP
        pl.semaphore_signal(barrier, inc=1, device_id=(peer, tp), device_id_type=MESH)
        pl.semaphore_signal(barrier, inc=1, device_id=(peer, other), device_id_type=MESH)
        return carry

    def greet_ring(i, carry):
        peer = 2 * ((z + i) % NZ) + core
        pl.semaphore_signal(barrier, inc=1, device_id=(ep, peer), device_id_type=MESH)
        return carry

    lax.fori_loop(1, NEP, greet_plane, 0)
    lax.fori_loop(1, NZ, greet_ring, 0)
    pl.semaphore_signal(barrier, inc=1, device_id=(ep, other), device_id_type=MESH)
    for copy in copies[12:]:
        copy.start()
    for copy in copies[:8]:
        copy.wait()

    eye = (
        lax.broadcasted_iota(jnp.int32, (ROWS, 128), 0)
        == lax.broadcasted_iota(jnp.int32, (ROWS, 128), 1)
    )

    inverse = v_table[HEADS : HEADS + 1, :]
    angle = v_pos[...].astype(F32) * inverse
    cosine = jnp.cos(angle)
    sine = jnp.sin(angle)
    lane = lax.broadcasted_iota(jnp.int32, (ROWS, 128), 1)
    sine = jnp.where(lane < HEAD // 2, -sine, sine)

    slot_expert = lane // 4
    first = v_ids[:, 0:1] == slot_expert
    second = v_ids[:, 1:2] == slot_expert
    named = jnp.where(first | second, 1.0, 0.0).astype(F32)
    earlier = jnp.where(
        lax.broadcasted_iota(jnp.int32, (ROWS, ROWS), 0)
        > lax.broadcasted_iota(jnp.int32, (ROWS, ROWS), 1),
        1.0,
        0.0,
    ).astype(BF16)
    ranks = jnp.dot(earlier, named.astype(BF16), preferred_element_type=F32)
    placed = jnp.where(ranks == (lane % 4).astype(F32), named, 0.0)
    combine = placed * jnp.where(first, v_weight[:, 0:1], v_weight[:, 1:2])
    del eye

    pl.semaphore_wait(barrier, 2 * (NEP - 1) + (NZ - 1) + 1)

    def copy_to(src, dst, send_sem, recv_sem, to_ep, to_tp):
        return pltpu.make_async_remote_copy(
            src_ref=src,
            dst_ref=dst,
            send_sem=send_sem,
            recv_sem=recv_sem,
            device_id=(to_ep, to_tp),
            device_id_type=MESH,
        )

    def a1_copy(i, slot):
        peer = 2 * ((z + ring_offset(i)) % NZ) + core
        return copy_to(v_hidden, agbuf.at[slot], a1_send.at[i], a1_recv.at[slot], ep, peer)

    def a1_start(i, carry):
        a1_copy(NZ - 2 - i, z).start()
        return carry

    lax.fori_loop(0, NZ - 1, a1_start, 0)

    def a2_copy(src, row, cc):
        return copy_to(
            src, xbuf.at[ep], a2_send.at[row, cc], a2_recv.at[ep], 2 * row + core, 2 * z + cc
        )

    def a2_from(src, row):
        target = 2 * row + core
        for cc in range(2):
            mine = (target == ep) & (cc == core)

            @pl.when(jnp.logical_not(mine))
            def _():
                a2_copy(src, row, cc).start()

            @pl.when(mine)
            def _():
                xbuf[pl.ds(ep, 1)] = src[...].reshape(1, ROWS, COLS)

    agbuf[pl.ds(z, 1)] = v_hidden[...].reshape(1, ROWS, COLS)
    a2_from(v_hidden, z)

    def a2_start(i, carry):
        row = (z + ring_offset(i)) % NZ
        a1_copy(i, row).wait_recv()
        a2_from(agbuf.at[row], row)
        return carry

    lax.fori_loop(0, NZ - 1, a2_start, 0)

    def square(i, total):
        part = agbuf[pl.ds(i, 1)].reshape(ROWS, COLS).astype(F32)
        part = part * part
        return total + part[:, :128] + part[:, 128:]

    ssout[...] = lax.fori_loop(0, NZ, square, jnp.zeros((ROWS, 128), F32))
    ss_copy = copy_to(ssout, ssin, ss_sem.at[0], ss_sem.at[1], ep, other)
    ss_copy.start()

    for copy in copies[8:12]:
        copy.wait()
    mix_row = v_mix_gain[:, pl.ds(pl.multiple_of(ep * COLS, COLS), COLS)]

    def plane_row(i):
        step = i + (i // 2) * (5 - 2 * i)
        return (ep // 4 + step) % 4

    def b_copy(slot, peer):
        return copy_to(bsend.at[peer], brecv.at[slot], b_send.at[peer], b_recv.at[slot], peer, tp)

    def b_rows(i, carry):
        row = plane_row(i)
        for k in range(4):
            peer = 4 * row + k

            @pl.when((peer != ep) | (ep % 2 != core))
            def _():
                copy_to(
                    v_hidden, xbuf.at[peer], a2_send.at[0, 0], a2_recv.at[peer], ep, other
                ).wait_recv()

        rows = xbuf[pl.ds(4 * row, 4)].astype(F32) * mix_row.reshape(1, 1, COLS)
        rows = rows.reshape(4 * ROWS, COLS).astype(BF16)
        sums = jnp.dot(rows, v_qkvg[...], preferred_element_type=F32)
        bsend[pl.ds(4 * row, 4)] = sums.reshape(4, ROWS, 512).astype(BF16)
        for k in range(4):
            peer = 4 * row + k

            @pl.when(peer != ep)
            def _():
                b_copy(ep, peer).start()

        return carry

    lax.fori_loop(0, 4, b_rows, 0)
    brecv[pl.ds(ep, 1)] = bsend[pl.ds(ep, 1)]

    ss_copy.wait_recv()
    square_sum = jnp.sum(ssout[...] + ssin[...], axis=-1, keepdims=True)
    factor = lax.rsqrt(square_sum * (1.0 / D) + EPS)

    def b_sum(i, total):
        row = plane_row(i)
        for k in range(4):
            peer = 4 * row + k

            @pl.when(peer != ep)
            def _():
                b_copy(peer, peer).wait_recv()

        part = brecv[pl.ds(4 * row, 4)].astype(F32)
        return total + ((part[0] + part[1]) + (part[2] + part[3]))

    joined = lax.fori_loop(0, 4, b_sum, jnp.zeros((ROWS, 512), F32))
    joined = (joined * factor).astype(BF16).astype(F32)

    def rotate(values):
        return values * cosine + pltpu.roll(values, HEAD // 2, 1) * sine

    rotated_query = rotate(joined[:, :128])
    rotated_key = rotate(joined[:, 128:256]) * HEAD ** (-0.5)
    value = joined[:, 256:384]
    gate_rows = joined[:, 384:]
    decay = v_table[pl.ds(tp, 1), :]
    readbuf[0] = rotated_query
    readbuf[1] = rotated_key
    readbuf[2] = value
    copies[12].wait()

    def retain(group, carry):
        at = pl.ds(pl.multiple_of(8 * group, 8), 8)
        query_columns = readbuf[0, at, :].T
        key_columns = readbuf[1, at, :].T
        values = readbuf[2, at, :]
        reads = []
        for k in range(8):
            state = (
                decay * v_state[8 * group + k, 0] + key_columns[:, k : k + 1] * values[k : k + 1, :]
            )
            v_state[8 * group + k, 0] = state
            reads.append(jnp.sum(query_columns[:, k : k + 1] * state, axis=0, keepdims=True))
        readbuf[3, at, :] = jnp.concatenate(reads, axis=0)
        return carry

    lax.fori_loop(0, ROWS // 8, retain, 0)
    state_out = pltpu.make_async_copy(v_state, next_state, local_sem.at[12])
    state_out.start()
    read = readbuf[3]
    centered = read - jnp.mean(read, axis=-1, keepdims=True)
    normal = centered * lax.rsqrt(jnp.mean(centered * centered, axis=-1, keepdims=True) + EPS)
    mixed = normal * v_head_gain[...] * jax.nn.silu(gate_rows)
    cbuf[pl.ds(tp, 1)] = mixed.astype(BF16).reshape(1, ROWS, HEAD)

    def gather(buf, send_sem, fwd_sem, recv_sem, consume):
        def direct(i, slot):
            peer = 2 * ((z + ring_offset(i)) % NZ) + core
            return copy_to(buf.at[slot], buf.at[slot], send_sem.at[i], recv_sem.at[slot], ep, peer)

        def forward(row, slot):
            return copy_to(
                buf.at[slot], buf.at[slot], fwd_sem.at[row], recv_sem.at[slot], ep, other
            )

        def begin(i, carry):
            direct(NZ - 2 - i, tp).start()
            return carry

        lax.fori_loop(0, NZ - 1, begin, 0)
        forward(z, tp).start()

        def step(i, carry):
            @pl.when(i < NZ - 1)
            def _():
                row = (z + ring_offset(i)) % NZ
                direct(0, 2 * row + core).wait_recv()
                forward(row, 2 * row + core).start()

            before = lax.select(i > 0, (z + ring_offset(lax.max(i - 1, 0))) % NZ, z)
            forward(before, 2 * before + 1 - core).wait_recv()
            consume(before, i == 0)
            return carry

        lax.fori_loop(0, NZ, step, 0)

        def finish():
            def one(i, carry):
                direct(i, tp).wait_send()
                forward((z + ring_offset(i)) % NZ, tp).wait_send()
                return carry

            lax.fori_loop(0, NZ - 1, one, 0)
            forward(z, tp).wait_send()

        return finish

    copies[13].wait()
    projected = readbuf.at[pl.ds(0, 2)]

    def project(row, first_step):
        pair = cbuf[pl.ds(2 * row, 2)].astype(F32)
        block = jnp.concatenate([pair[0], pair[1]], axis=1).astype(BF16)
        part = jnp.dot(
            block,
            v_out[pl.ds(pl.multiple_of(row * COLS, COLS), COLS), :],
            preferred_element_type=F32,
        )

        @pl.when(first_step)
        def _():
            projected[0] = part[:, :128]
            projected[1] = part[:, 128:]

        @pl.when(jnp.logical_not(first_step))
        def _():
            projected[0] += part[:, :128]
            projected[1] += part[:, 128:]

    finish_c = gather(cbuf, c_send, c_fwd, c_recv, project)
    own = v_hidden[...].astype(F32)
    after = (own + jnp.concatenate([projected[0], projected[1]], axis=1)).astype(BF16)

    packed = lax.dot_general(
        placed.astype(BF16), after, (((0,), (0,)), ((), ())), preferred_element_type=F32
    )

    def halves_below(array):
        parts = [array[:, :128].reshape(NEP, 8, 128), array[:, 128:].reshape(NEP, 8, 128)]
        return jnp.concatenate(parts, axis=1)

    def halves_beside(array):
        array = array.astype(F32)
        return array[:, :8].reshape(SLOTS, 128), array[:, 8:].reshape(SLOTS, 128)

    psend[...] = halves_below(packed).astype(BF16)

    def d1_copy(peer, source):
        return copy_to(
            psend.at[peer], dbuf.at[tp, source], d1_send.at[peer], d1_recv.at[source], peer, tp
        )

    def d1_start(i, carry):
        d1_copy((ep + i) % NEP, ep).start()
        return carry

    lax.fori_loop(1, NEP, d1_start, 0)
    dbuf[pl.ds(tp, 1), pl.ds(ep, 1)] = psend[pl.ds(ep, 1)].reshape(1, 1, 16, 128)

    def d1_wait(i, carry):
        peer = (ep + i) % NEP
        d1_copy(peer, peer).wait_recv()
        return carry

    lax.fori_loop(1, NEP, d1_wait, 0)
    copies[14].wait()
    copies[15].wait()

    square_of = acc_gu.at[2]

    def lift(row, first_step):
        @pl.when(first_step)
        def _():
            acc_gu[...] = jnp.zeros_like(acc_gu)

        for k in range(2):
            slot = 2 * row + k
            at = pl.multiple_of(slot * COLS, COLS)
            low, high = halves_beside(dbuf[pl.ds(slot, 1)].reshape(NEP, 16, 128))
            square_of[:, :128] += low * low + high * high
            both = jnp.concatenate([low, high], axis=1) * v_ffn_gain[:, pl.ds(at, COLS)]
            both = both.astype(BF16)
            for j in range(2):
                acc_gu[j] += jnp.dot(both, v_gu[j, pl.ds(at, COLS), :], preferred_element_type=F32)

    finish_d = gather(dbuf, d_send, d_fwd, d_recv, lift)
    inner = lax.rsqrt(
        jnp.sum(square_of[:, :128], axis=-1, keepdims=True) * (1.0 / D) + EPS
    )
    own_expert = lax.broadcasted_iota(jnp.int32, (SLOTS, COLS), 0) % 8 < 4
    chosen = jnp.where(own_expert, acc_gu[0], acc_gu[1]) * inner
    activated = jax.nn.silu(chosen[:, :128]) * chosen[:, 128:]
    ebuf[pl.ds(tp, 1)] = activated.astype(BF16).reshape(1, SLOTS, 128)
    copies[16].wait()

    def lower(row, first_step):
        @pl.when(first_step)
        def _():
            acc_down[...] = jnp.zeros_like(acc_down)

        pair = ebuf[pl.ds(2 * row, 2)]
        both = jnp.concatenate([pair[0], pair[1]], axis=1)
        at = pl.multiple_of(row * COLS, COLS)
        for j in range(2):
            acc_down[j] += jnp.dot(both, v_down[j, pl.ds(at, COLS), :], preferred_element_type=F32)

    finish_e = gather(ebuf, e_send, e_fwd, e_recv, lower)
    result = jnp.where(own_expert, acc_down[0], acc_down[1])

    fsend[...] = halves_below(result).astype(BF16)

    def f_copy(peer, source):
        return copy_to(
            fsend.at[peer], frecv.at[source], f_send.at[peer], f_recv.at[source], peer, tp
        )

    def f_start(i, carry):
        f_copy((ep + i) % NEP, ep).start()
        return carry

    lax.fori_loop(1, NEP, f_start, 0)
    frecv[pl.ds(ep, 1)] = fsend[pl.ds(ep, 1)]

    def sent_ring(i, carry):
        a1_copy(i, z).wait_send()
        return carry

    lax.fori_loop(0, NZ - 1, sent_ring, 0)

    def sent_a2(row, carry):
        for cc in range(2):

            @pl.when((2 * row + core != ep) | (cc != core))
            def _():
                a2_copy(v_hidden, row, cc).wait_send()

        return carry

    lax.fori_loop(0, NZ, sent_a2, 0)
    ss_copy.wait_send()

    def sent_plane(i, carry):
        peer = (ep + i) % NEP
        b_copy(ep, peer).wait_send()
        d1_copy(peer, ep).wait_send()
        return carry

    lax.fori_loop(1, NEP, sent_plane, 0)
    finish_c()
    finish_d()
    finish_e()

    def f_wait(i, carry):
        peer = (ep + i) % NEP
        f_copy(peer, peer).wait_recv()
        return carry

    lax.fori_loop(1, NEP, f_wait, 0)
    back = jnp.concatenate(halves_beside(frecv[...]), axis=1)
    weighted = jnp.dot(
        combine, back, preferred_element_type=F32, precision=lax.Precision.HIGHEST
    )
    updated[...] = (after.astype(F32) + weighted).astype(BF16)

    def f_sent(i, carry):
        f_copy((ep + i) % NEP, ep).wait_send()
        return carry

    lax.fori_loop(1, NEP, f_sent, 0)
    state_out.wait()


def per_device(
    hidden,
    positions,
    ret_state,
    query_weight,
    key_weight,
    value_weight,
    gate_weight,
    head_gain,
    out_weight,
    mix_gain,
    ffn_gain,
    expert_gate,
    expert_up,
    expert_down,
    route_ids,
    route_weight,
):
    dma = pltpu.SemaphoreType.DMA
    vmem = pltpu.VMEM
    anywhere = pl.BlockSpec(memory_space=pl.ANY)
    return pl.pallas_call(
        body,
        out_shape=(
            jax.ShapeDtypeStruct((ROWS, COLS), BF16),
            jax.ShapeDtypeStruct(ret_state.shape, F32),
        ),
        in_specs=[anywhere] * 17,
        out_specs=(pl.BlockSpec(memory_space=pltpu.VMEM), anywhere),
        scratch_shapes=[
            vmem((ROWS, COLS), BF16),
            vmem((ROWS, 1), jnp.int32),
            vmem((ROWS, 1, HEAD, HEAD), F32),
            vmem((COLS, 512), BF16),
            vmem((1, HEAD), F32),
            vmem((RD, COLS), BF16),
            vmem((1, D), F32),
            vmem((1, D), F32),
            vmem((2, D, COLS), BF16),
            vmem((2, RD, COLS), BF16),
            vmem((ROWS, 2), jnp.int32),
            vmem((ROWS, 2), F32),
            vmem((24, 128), F32),
            vmem((NZ, ROWS, COLS), BF16),
            vmem((NEP, ROWS, COLS), BF16),
            vmem((NEP, ROWS, 512), BF16),
            vmem((NEP, ROWS, 512), BF16),
            vmem((ROWS, 128), F32),
            vmem((ROWS, 128), F32),
            vmem((4, ROWS, HEAD), F32),
            vmem((NTP, ROWS, HEAD), BF16),
            vmem((NEP, 16, 128), BF16),
            vmem((NTP, NEP, 16, 128), BF16),
            vmem((3, SLOTS, COLS), F32),
            vmem((NTP, SLOTS, 128), BF16),
            vmem((2, SLOTS, COLS), F32),
            vmem((NEP, 16, 128), BF16),
            vmem((NEP, 16, 128), BF16),
            dma((17,)),
            dma((NZ,)),
            dma((NZ,)),
            dma((NZ, 2)),
            dma((NEP,)),
            dma((2,)),
            dma((NEP,)),
            dma((NEP,)),
            dma((NZ,)),
            dma((NZ,)),
            dma((NTP,)),
            dma((NEP,)),
            dma((NEP,)),
            dma((NZ,)),
            dma((NZ,)),
            dma((NTP,)),
            dma((NZ,)),
            dma((NZ,)),
            dma((NTP,)),
            dma((NEP,)),
            dma((NEP,)),
        ],
        compiler_params=pltpu.CompilerParams(
            collective_id=0, has_side_effects=True, vmem_limit_bytes=48 * 1024 * 1024
        ),
    )(
        hidden,
        positions.reshape(ROWS, 1),
        ret_state,
        query_weight,
        key_weight,
        value_weight,
        gate_weight,
        head_gain.reshape(1, HEAD),
        out_weight,
        mix_gain.reshape(1, D),
        ffn_gain.reshape(1, D),
        expert_gate,
        expert_up,
        expert_down,
        route_ids,
        route_weight,
        jnp.asarray(constants()),
    )


def solution(mesh):
    return jax.shard_map(
        per_device,
        mesh=mesh,
        in_specs=(
            P("ep", "tp"),
            P("ep"),
            P("ep", "tp", None, None),
            P("ep", "tp"),
            P("ep", "tp"),
            P("ep", "tp"),
            P("ep", "tp"),
            P("tp"),
            P(None, "tp"),
            P(),
            P(),
            P("ep", None, "tp"),
            P("ep", None, "tp"),
            P("ep", None, "tp"),
            P("ep", None),
            P("ep", None),
        ),
        out_specs=(P("ep", "tp"), P("ep", "tp", None, None)),
        check_vma=False,
    )
```

```python
import functools

import jax
import jax.numpy as jnp
import numpy as np
from jax import lax
from jax.experimental import pallas as pl
from jax.experimental.pallas import tpu as pltpu
from jax.sharding import PartitionSpec as P

MESH = pl.DeviceIdType.MESH
F32 = jnp.float32
BF16 = jnp.bfloat16
D = 4096
RD = 2048
HEADS = 16
HEAD = 128
ROWS = 40
COLS = 256
NEP = 16
NTP = 16
NZ = 8
SLOTS = 128
GROUPS_OF_ROWS = ROWS // 8
EPS = 1e-06


def constants():
    table = np.zeros((24, 128), np.float64)
    heads = np.arange(HEADS, dtype=np.float64)
    table[:HEADS] = (1.0 - 2.0 ** (-5.0 - 5.0 * heads / (HEADS - 1)))[:, None]
    inverse = 10000.0 ** (-np.arange(0, HEAD, 2, dtype=np.float64) / HEAD)
    table[HEADS] = np.concatenate([inverse, inverse])
    return table.astype(np.float32)


TRACE = False
_open = []


def mark(name):
    if not TRACE:
        return
    while _open:
        _open.pop().__exit__(None, None, None)
    if name:
        _open.append(jax.named_scope(name))
        _open[-1].__enter__()


def ring_offset(i):
    half = i // 2 + 1
    return half + (i % 2) * (NZ - 2 * half)


def body(
    hidden,
    positions,
    ret_state,
    query_weight,
    key_weight,
    value_weight,
    gate_weight,
    head_gain,
    out_weight,
    mix_gain,
    ffn_gain,
    expert_gate,
    expert_up,
    expert_down,
    route_ids,
    route_weight,
    table,
    updated,
    state_parts,
    v_hidden,
    v_pos,
    v_state,
    v_qkvg,
    v_head_gain,
    v_out,
    v_mix_gain,
    v_ffn_gain,
    v_gu,
    v_down,
    v_ids,
    v_weight,
    v_table,
    agbuf,
    xbuf,
    bsend,
    brecv,
    ssout,
    ssin,
    readbuf,
    cbuf,
    afters,
    psend,
    dbuf,
    acc_gu,
    ebuf,
    acc_down,
    fsend,
    frecv,
    local_sem,
    a1_send,
    a1_recv,
    a2_send,
    a2_recv,
    ss_sem,
    b_send,
    b_recv,
    c_send,
    c_fwd,
    c_recv,
    g_send,
    g_recv,
    d_send,
    d_fwd,
    d_recv,
    d_other,
    e_send,
    e_fwd,
    e_recv,
    f_send,
    f_recv,
):
    ep = lax.axis_index("ep")
    tp = lax.axis_index("tp")
    z = tp // 2
    core = tp % 2
    other = 2 * z + 1 - core

    mark("load")
    loads = [
        (hidden, v_hidden),
        (positions, v_pos),
        (table, v_table),
        (route_ids, v_ids),
        (route_weight, v_weight),
        (head_gain, v_head_gain),
        (mix_gain, v_mix_gain),
        (ffn_gain, v_ffn_gain),
        (query_weight, v_qkvg.at[:, pl.ds(0, 128)]),
        (key_weight, v_qkvg.at[:, pl.ds(128, 128)]),
        (value_weight, v_qkvg.at[:, pl.ds(256, 128)]),
        (gate_weight, v_qkvg.at[:, pl.ds(384, 128)]),
        (ret_state, v_state),
        (out_weight, v_out),
        (expert_gate, v_gu.at[:, :, pl.ds(0, 128)]),
        (expert_up, v_gu.at[:, :, pl.ds(128, 128)]),
        (expert_down, v_down),
    ]
    copies = [pltpu.make_async_copy(src, dst, local_sem.at[i]) for i, (src, dst) in enumerate(loads)]
    for copy in copies[:12]:
        copy.start()

    barrier = pltpu.get_barrier_semaphore()

    def greet_plane(i, carry):
        peer = (ep + i) % NEP
        pl.semaphore_signal(barrier, inc=1, device_id=(peer, tp), device_id_type=MESH)
        pl.semaphore_signal(barrier, inc=1, device_id=(peer, other), device_id_type=MESH)
        return carry

    def greet_ring(i, carry):
        peer = 2 * ((z + i) % NZ) + core
        pl.semaphore_signal(barrier, inc=1, device_id=(ep, peer), device_id_type=MESH)
        return carry

    lax.fori_loop(1, NEP, greet_plane, 0)
    lax.fori_loop(1, NZ, greet_ring, 0)
    pl.semaphore_signal(barrier, inc=1, device_id=(ep, other), device_id_type=MESH)
    for copy in copies[12:]:
        copy.start()
    for copy in copies[:8]:
        copy.wait()

    mark("prep")
    token = lax.broadcasted_iota(jnp.int32, (ROWS, ROWS), 0)
    other_token = lax.broadcasted_iota(jnp.int32, (ROWS, ROWS), 1)

    def column(row):
        return jnp.sum(jnp.where(token == other_token, row.astype(F32), 0.0), axis=1, keepdims=True)

    inverse = v_table[HEADS : HEADS + 1, :]
    angle = column(v_pos[...]) * inverse
    cosine = jnp.cos(angle)
    sine = jnp.sin(angle)
    lane = lax.broadcasted_iota(jnp.int32, (ROWS, 128), 1)
    sine = jnp.where(lane < HEAD // 2, -sine, sine)

    slot_expert = lane // 4
    slot_expert = slot_expert.astype(F32)
    first = column(v_ids[0:1, :]) == slot_expert
    second = column(v_ids[1:2, :]) == slot_expert
    named = jnp.where(first | second, 1.0, 0.0).astype(F32)
    earlier = jnp.where(token > other_token, 1.0, 0.0).astype(BF16)
    ranks = jnp.dot(earlier, named.astype(BF16), preferred_element_type=F32)
    placed = jnp.where(ranks == (lane % 4).astype(F32), named, 0.0)
    combine = placed * jnp.where(first, column(v_weight[0:1, :]), column(v_weight[1:2, :]))

    mark("barrier")
    pl.semaphore_wait(barrier, 2 * (NEP - 1) + (NZ - 1) + 1)

    def copy_to(src, dst, send_sem, recv_sem, to_ep, to_tp):
        return pltpu.make_async_remote_copy(
            src_ref=src,
            dst_ref=dst,
            send_sem=send_sem,
            recv_sem=recv_sem,
            device_id=(to_ep, to_tp),
            device_id_type=MESH,
        )

    def a1_copy(i, slot):
        peer = 2 * ((z + ring_offset(i)) % NZ) + core
        return copy_to(v_hidden, agbuf.at[slot], a1_send.at[i], a1_recv.at[slot], ep, peer)

    def a1_start(i, carry):
        a1_copy(NZ - 2 - i, z).start()
        return carry

    mark("a1_issue")
    lax.fori_loop(0, NZ - 1, a1_start, 0)

    def a2_copy(src, row, cc):
        return copy_to(
            src, xbuf.at[ep], a2_send.at[row, cc], a2_recv.at[ep], 2 * row + core, 2 * z + cc
        )

    def a2_from(src, row):
        target = 2 * row + core
        for cc in range(2):
            mine = (target == ep) & (cc == core)

            @pl.when(jnp.logical_not(mine))
            def _():
                a2_copy(src, row, cc).start()

            @pl.when(mine)
            def _():
                xbuf[pl.ds(ep, 1)] = src[...].reshape(1, ROWS, COLS)

    agbuf[pl.ds(z, 1)] = v_hidden[...].reshape(1, ROWS, COLS)
    a2_from(v_hidden, z)

    def a2_start(i, carry):
        row = (z + ring_offset(i)) % NZ
        a1_copy(i, row).wait_recv()
        a2_from(agbuf.at[row], row)
        return carry

    mark("a1_wait_a2_issue")
    lax.fori_loop(0, NZ - 1, a2_start, 0)

    mark("ss")
    def square(i, total):
        part = agbuf[pl.ds(i, 1)].reshape(ROWS, COLS).astype(F32)
        part = part * part
        return total + part[:, :128] + part[:, 128:]

    ssout[...] = lax.fori_loop(0, NZ, square, jnp.zeros((ROWS, 128), F32))
    ss_copy = copy_to(ssout, ssin, ss_sem.at[0], ss_sem.at[1], ep, other)
    ss_copy.start()

    for copy in copies[8:12]:
        copy.wait()
    mix_row = v_mix_gain[:, pl.ds(pl.multiple_of(ep * COLS, COLS), COLS)]

    def plane_peer(i):
        down, along = i // 4, i % 4
        down = down + (down // 2) * (5 - 2 * down)
        along = along + (along // 2) * (5 - 2 * along)
        return ((ep // 4 + down) % 4) * 4 + (ep + along) % 4

    def plane_row(i):
        step = i + (i // 2) * (5 - 2 * i)
        return (ep // 4 + step) % 4

    def b_copy(slot, peer):
        return copy_to(bsend.at[peer], brecv.at[slot], b_send.at[peer], b_recv.at[slot], peer, tp)

    def b_rows(i, carry):
        row = plane_row(i)
        for k in range(4):
            peer = 4 * row + k

            @pl.when((peer != ep) | (ep % 2 != core))
            def _():
                copy_to(
                    v_hidden, xbuf.at[peer], a2_send.at[0, 0], a2_recv.at[peer], ep, other
                ).wait_recv()

        rows = xbuf[pl.ds(4 * row, 4)].astype(F32) * mix_row.reshape(1, 1, COLS)
        rows = rows.reshape(4 * ROWS, COLS).astype(BF16)
        sums = jnp.dot(rows, v_qkvg[...], preferred_element_type=F32)
        bsend[pl.ds(4 * row, 4)] = sums.reshape(4, ROWS, 512).astype(BF16)
        for k in range(4):
            peer = 4 * row + k

            @pl.when(peer != ep)
            def _():
                b_copy(ep, peer).start()

        return carry

    mark("b_rows")
    lax.fori_loop(0, 4, b_rows, 0)
    brecv[pl.ds(ep, 1)] = bsend[pl.ds(ep, 1)]

    mark("ss_wait")
    ss_copy.wait_recv()
    square_sum = jnp.sum(ssout[...] + ssin[...], axis=-1, keepdims=True)
    factor = lax.rsqrt(square_sum * (1.0 / D) + EPS)

    def b_sum(i, total):
        row = plane_row(i)
        for k in range(4):
            peer = 4 * row + k

            @pl.when(peer != ep)
            def _():
                b_copy(peer, peer).wait_recv()

        part = brecv[pl.ds(4 * row, 4)].astype(F32)
        return total + ((part[0] + part[1]) + (part[2] + part[3]))

    mark("b_sum")
    joined = lax.fori_loop(0, 4, b_sum, jnp.zeros((ROWS, 512), F32))
    joined = (joined * factor).astype(BF16).astype(F32)

    mark("rot")
    def rotate(values):
        return values * cosine + pltpu.roll(values, HEAD // 2, 1) * sine

    rotated_query = rotate(joined[:, :128])
    rotated_key = rotate(joined[:, 128:256]) * HEAD ** (-0.5)
    value = joined[:, 256:384]
    gate_rows = joined[:, 384:]
    decay = v_table[pl.ds(tp, 1), :]
    readbuf[0] = rotated_query
    readbuf[1] = rotated_key
    readbuf[2] = value
    state_parts[0] = rotated_key
    state_parts[1] = value
    mark("retain")
    copies[12].wait()

    def retain(group, carry):
        at = pl.ds(pl.multiple_of(8 * group, 8), 8)
        query_columns = readbuf[0, at, :].T
        key_columns = readbuf[1, at, :].T
        values = readbuf[2, at, :]
        reads = []
        for k in range(8):
            state = (
                decay * v_state[8 * group + k, 0] + key_columns[:, k : k + 1] * values[k : k + 1, :]
            )
            reads.append(jnp.sum(query_columns[:, k : k + 1] * state, axis=0, keepdims=True))
        readbuf[3, at, :] = jnp.concatenate(reads, axis=0)
        return carry

    lax.fori_loop(0, ROWS // 8, retain, 0)
    mark("groupnorm")
    read = readbuf[3]
    centered = read - jnp.mean(read, axis=-1, keepdims=True)
    normal = centered * lax.rsqrt(jnp.mean(centered * centered, axis=-1, keepdims=True) + EPS)
    mixed = normal * v_head_gain[...] * jax.nn.silu(gate_rows)
    cbuf[pl.ds(tp, 1)] = mixed.astype(BF16).reshape(1, ROWS, HEAD)

    def gather(buf, send_sem, fwd_sem, recv_sem, consume):
        def direct(i, slot):
            peer = 2 * ((z + ring_offset(i)) % NZ) + core
            return copy_to(buf.at[slot], buf.at[slot], send_sem.at[i], recv_sem.at[slot], ep, peer)

        def forward(row, slot):
            return copy_to(
                buf.at[slot], buf.at[slot], fwd_sem.at[row], recv_sem.at[slot], ep, other
            )

        def begin(i, carry):
            direct(NZ - 2 - i, tp).start()
            return carry

        lax.fori_loop(0, NZ - 1, begin, 0)
        forward(z, tp).start()

        def step(i, carry):
            @pl.when(i < NZ - 1)
            def _():
                row = (z + ring_offset(i)) % NZ
                direct(0, 2 * row + core).wait_recv()
                forward(row, 2 * row + core).start()

            before = lax.select(i > 0, (z + ring_offset(lax.max(i - 1, 0))) % NZ, z)
            forward(before, 2 * before + 1 - core).wait_recv()
            consume(before, i == 0)
            return carry

        lax.fori_loop(0, NZ, step, 0)

        def finish():
            def one(i, carry):
                direct(i, tp).wait_send()
                forward((z + ring_offset(i)) % NZ, tp).wait_send()
                return carry

            lax.fori_loop(0, NZ - 1, one, 0)
            forward(z, tp).wait_send()

        return finish

    copies[13].wait()
    projected = readbuf.at[pl.ds(0, 2)]

    def project(row, first_step):
        pair = cbuf[pl.ds(2 * row, 2)].astype(F32)
        block = jnp.concatenate([pair[0], pair[1]], axis=1).astype(BF16)
        part = jnp.dot(
            block,
            v_out[pl.ds(pl.multiple_of(row * COLS, COLS), COLS), :],
            preferred_element_type=F32,
        )

        @pl.when(first_step)
        def _():
            projected[0] = part[:, :128]
            projected[1] = part[:, 128:]

        @pl.when(jnp.logical_not(first_step))
        def _():
            projected[0] += part[:, :128]
            projected[1] += part[:, 128:]

    mark("c_gather")
    finish_c = gather(cbuf, c_send, c_fwd, c_recv, project)
    mark("after_pack")
    own = v_hidden[...].astype(F32)
    after = (own + jnp.concatenate([projected[0], projected[1]], axis=1)).astype(BF16)
    afters[pl.ds(z, 1)] = after.reshape(1, ROWS, COLS)

    def g_copy(i, slot):
        peer = 2 * ((z + ring_offset(i)) % NZ) + core
        return copy_to(afters.at[z], afters.at[slot], g_send.at[i], g_recv.at[slot], ep, peer)

    def g_start(i, carry):
        g_copy(NZ - 2 - i, z).start()
        return carry

    lax.fori_loop(0, NZ - 1, g_start, 0)

    def halves_below(array):
        parts = [array[:, :128].reshape(NEP, 8, 128), array[:, 128:].reshape(NEP, 8, 128)]
        return jnp.concatenate(parts, axis=1)

    def halves_beside(array):
        array = array.astype(F32)
        return array[:, :8].reshape(SLOTS, 128), array[:, 8:].reshape(SLOTS, 128)

    placing = placed.astype(BF16)

    def pack(row):
        packed = lax.dot_general(
            placing,
            afters[pl.ds(row, 1)].reshape(ROWS, COLS),
            (((0,), (0,)), ((), ())),
            preferred_element_type=F32,
        )
        psend[:, pl.ds(row, 1)] = halves_below(packed).astype(BF16).reshape(NEP, 1, 16, 128)

    pack(z)

    def pack_next(i, carry):
        row = (z + ring_offset(i)) % NZ
        g_copy(i, row).wait_recv()
        pack(row)
        return carry

    mark("after_gather")
    lax.fori_loop(0, NZ - 1, pack_next, 0)

    def d_copy(peer, source):
        return copy_to(
            psend.at[peer], dbuf.at[core, source], d_send.at[peer], d_recv.at[source], peer, tp
        )

    def d_forward(parity, source):
        block = dbuf.at[parity, source]
        return copy_to(block, block, d_fwd.at[source], d_other.at[source], ep, other)

    def d_start(i, carry):
        d_copy(plane_peer(NEP - 1 - i), ep).start()
        return carry

    mark("d_issue")
    lax.fori_loop(0, NEP - 1, d_start, 0)
    dbuf[pl.ds(core, 1), pl.ds(ep, 1)] = psend[pl.ds(ep, 1)].reshape(1, 1, NZ, 16, 128)
    d_forward(core, ep).start()

    def d_arrive(i, carry):
        peer = plane_peer(i)
        d_copy(peer, peer).wait_recv()
        d_forward(core, peer).start()
        return carry

    acc_gu[...] = jnp.zeros_like(acc_gu)
    mark("d_wait")
    lax.fori_loop(1, NEP, d_arrive, 0)
    copies[14].wait()
    copies[15].wait()
    square_of = acc_gu.at[2]

    def lift(parity):
        def one(row, carry):
            at = pl.multiple_of((2 * row + parity) * COLS, COLS)
            block = dbuf[pl.ds(parity, 1), :, pl.ds(row, 1)].reshape(NEP, 16, 128)
            low, high = halves_beside(block)
            square_of[:, :128] += low * low + high * high
            both = jnp.concatenate([low, high], axis=1) * v_ffn_gain[:, pl.ds(at, COLS)]
            both = both.astype(BF16)
            for j in range(2):
                acc_gu[j] += jnp.dot(both, v_gu[j, pl.ds(at, COLS), :], preferred_element_type=F32)
            return carry

        lax.fori_loop(0, NZ, one, 0)

    mark("lift_own")
    lift(core)

    def d_other_wait(source, carry):
        d_forward(1 - core, source).wait_recv()
        return carry

    mark("lift_wait")
    lax.fori_loop(0, NEP, d_other_wait, 0)
    mark("lift_other")
    lift(1 - core)
    mark("act")
    inner = lax.rsqrt(
        jnp.sum(square_of[:, :128], axis=-1, keepdims=True) * (1.0 / D) + EPS
    )
    own_expert = lax.broadcasted_iota(jnp.int32, (SLOTS, COLS), 0) % 8 < 4
    chosen = jnp.where(own_expert, acc_gu[0], acc_gu[1]) * inner
    activated = jax.nn.silu(chosen[:, :128]) * chosen[:, 128:]
    ebuf[pl.ds(tp, 1)] = activated.astype(BF16).reshape(1, SLOTS, 128)
    copies[16].wait()

    def lower(row, first_step):
        @pl.when(first_step)
        def _():
            acc_down[...] = jnp.zeros_like(acc_down)

        pair = ebuf[pl.ds(2 * row, 2)]
        both = jnp.concatenate([pair[0], pair[1]], axis=1)
        at = pl.multiple_of(row * COLS, COLS)
        for j in range(2):
            acc_down[j] += jnp.dot(both, v_down[j, pl.ds(at, COLS), :], preferred_element_type=F32)

    mark("e_gather")
    finish_e = gather(ebuf, e_send, e_fwd, e_recv, lower)
    mark("result")
    result = jnp.where(own_expert, acc_down[0], acc_down[1])

    fsend[...] = halves_below(result).astype(BF16)

    def f_copy(peer, source):
        return copy_to(
            fsend.at[peer], frecv.at[source], f_send.at[peer], f_recv.at[source], peer, tp
        )

    def f_start(i, carry):
        f_copy((ep + i) % NEP, ep).start()
        return carry

    lax.fori_loop(1, NEP, f_start, 0)
    frecv[pl.ds(ep, 1)] = fsend[pl.ds(ep, 1)]

    mark("sent")
    def sent_ring(i, carry):
        a1_copy(i, z).wait_send()
        g_copy(i, z).wait_send()
        return carry

    lax.fori_loop(0, NZ - 1, sent_ring, 0)

    def sent_a2(row, carry):
        for cc in range(2):

            @pl.when((2 * row + core != ep) | (cc != core))
            def _():
                a2_copy(v_hidden, row, cc).wait_send()

        return carry

    lax.fori_loop(0, NZ, sent_a2, 0)
    ss_copy.wait_send()
    d_forward(core, ep).wait_send()

    def sent_plane(i, carry):
        peer = (ep + i) % NEP
        b_copy(ep, peer).wait_send()
        d_copy(peer, ep).wait_send()
        d_forward(core, peer).wait_send()
        return carry

    lax.fori_loop(1, NEP, sent_plane, 0)
    finish_c()
    finish_e()

    def f_wait(i, carry):
        peer = (ep + i) % NEP
        f_copy(peer, peer).wait_recv()
        return carry

    mark("f_wait")
    lax.fori_loop(1, NEP, f_wait, 0)
    mark("combine")
    back = jnp.concatenate(halves_beside(frecv[...]), axis=1)
    weighted = jnp.dot(
        combine, back, preferred_element_type=F32, precision=lax.Precision.HIGHEST
    )
    updated[...] = (after.astype(F32) + weighted).astype(BF16)

    def f_sent(i, carry):
        f_copy((ep + i) % NEP, ep).wait_send()
        return carry

    lax.fori_loop(1, NEP, f_sent, 0)
    mark("")


def state_body(
    before, parts, table, ret_state, updated, next_state, v_updated, v_parts, v_table, v_state, sem, load, store
):
    copies = [
        pltpu.make_async_copy(parts, v_parts, sem.at[0]),
        pltpu.make_async_copy(table, v_table, sem.at[1]),
        pltpu.make_async_copy(before, v_updated, sem.at[2]),
    ]
    out = pltpu.make_async_copy(v_updated, updated, sem.at[3])

    def rows_in(group):
        at = pl.ds(8 * group, 8)
        return pltpu.make_async_copy(ret_state.at[at], v_state.at[at], load.at[group])

    def rows_out(group):
        at = pl.ds(8 * group, 8)
        return pltpu.make_async_copy(v_state.at[at], next_state.at[at], store.at[group])

    for copy in copies:
        copy.start()
    for group in range(GROUPS_OF_ROWS):
        rows_in(group).start()
    for copy in copies:
        copy.wait()
    out.start()
    decay = v_table[pl.ds(lax.axis_index("tp"), 1), :]

    def one(group, carry):
        at = pl.ds(pl.multiple_of(8 * group, 8), 8)
        key_columns = v_parts[0, at, :].T
        values = v_parts[1, at, :]
        rows_in(group).wait()
        for k in range(8):
            v_state[8 * group + k, 0] = (
                decay * v_state[8 * group + k, 0] + key_columns[:, k : k + 1] * values[k : k + 1, :]
            )
        rows_out(group).start()
        return carry

    lax.fori_loop(0, GROUPS_OF_ROWS, one, 0)
    out.wait()
    for group in range(GROUPS_OF_ROWS):
        rows_out(group).wait()


def per_device(
    hidden,
    positions,
    ret_state,
    query_weight,
    key_weight,
    value_weight,
    gate_weight,
    head_gain,
    out_weight,
    mix_gain,
    ffn_gain,
    expert_gate,
    expert_up,
    expert_down,
    route_ids,
    route_weight,
):
    table = jnp.asarray(constants())
    dma = pltpu.SemaphoreType.DMA
    vmem = pltpu.VMEM
    anywhere = pl.BlockSpec(memory_space=pltpu.HBM)
    updated, parts = pl.pallas_call(
        body,
        out_shape=(
            jax.ShapeDtypeStruct((ROWS, COLS), BF16),
            jax.ShapeDtypeStruct((2, ROWS, HEAD), F32),
        ),
        in_specs=[anywhere] * 17,
        out_specs=(pl.BlockSpec(memory_space=pltpu.VMEM),) * 2,
        scratch_shapes=[
            vmem((ROWS, COLS), BF16),
            vmem((1, ROWS), jnp.int32),
            vmem((ROWS, 1, HEAD, HEAD), F32),
            vmem((COLS, 512), BF16),
            vmem((1, HEAD), F32),
            vmem((RD, COLS), BF16),
            vmem((1, D), F32),
            vmem((1, D), F32),
            vmem((2, D, COLS), BF16),
            vmem((2, RD, COLS), BF16),
            vmem((2, ROWS), jnp.int32),
            vmem((2, ROWS), F32),
            vmem((24, 128), F32),
            vmem((NZ, ROWS, COLS), BF16),
            vmem((NEP, ROWS, COLS), BF16),
            vmem((NEP, ROWS, 512), BF16),
            vmem((NEP, ROWS, 512), BF16),
            vmem((ROWS, 128), F32),
            vmem((ROWS, 128), F32),
            vmem((4, ROWS, HEAD), F32),
            vmem((NTP, ROWS, HEAD), BF16),
            vmem((NZ, ROWS, COLS), BF16),
            vmem((NEP, NZ, 16, 128), BF16),
            vmem((2, NEP, NZ, 16, 128), BF16),
            vmem((3, SLOTS, COLS), F32),
            vmem((NTP, SLOTS, 128), BF16),
            vmem((2, SLOTS, COLS), F32),
            vmem((NEP, 16, 128), BF16),
            vmem((NEP, 16, 128), BF16),
            dma((17,)),
            dma((NZ,)),
            dma((NZ,)),
            dma((NZ, 2)),
            dma((NEP,)),
            dma((2,)),
            dma((NEP,)),
            dma((NEP,)),
            dma((NZ,)),
            dma((NZ,)),
            dma((NTP,)),
            dma((NZ,)),
            dma((NZ,)),
            dma((NEP,)),
            dma((NEP,)),
            dma((NEP,)),
            dma((NEP,)),
            dma((NZ,)),
            dma((NZ,)),
            dma((NTP,)),
            dma((NEP,)),
            dma((NEP,)),
        ],
        compiler_params=pltpu.CompilerParams(
            collective_id=0, has_side_effects=True, vmem_limit_bytes=67043328
        ),
    )(
        hidden,
        positions.reshape(1, ROWS),
        ret_state,
        query_weight,
        key_weight,
        value_weight,
        gate_weight,
        head_gain.reshape(1, HEAD),
        out_weight,
        mix_gain.reshape(1, D),
        ffn_gain.reshape(1, D),
        expert_gate,
        expert_up,
        expert_down,
        route_ids.T,
        route_weight.T,
        table,
    )
    return pl.pallas_call(
        state_body,
        out_shape=(
            jax.ShapeDtypeStruct((ROWS, COLS), BF16),
            jax.ShapeDtypeStruct(ret_state.shape, F32),
        ),
        in_specs=[anywhere] * 4,
        out_specs=(anywhere,) * 2,
        scratch_shapes=[
            vmem((ROWS, COLS), BF16),
            vmem((2, ROWS, HEAD), F32),
            vmem((24, 128), F32),
            vmem((ROWS, 1, HEAD, HEAD), F32),
            dma((4,)),
            dma((GROUPS_OF_ROWS,)),
            dma((GROUPS_OF_ROWS,)),
        ],
        compiler_params=pltpu.CompilerParams(vmem_limit_bytes=67043328),
    )(updated, parts, table, ret_state)


def solution(mesh):
    return jax.shard_map(
        per_device,
        mesh=mesh,
        in_specs=(
            P("ep", "tp"),
            P("ep"),
            P("ep", "tp", None, None),
            P("ep", "tp"),
            P("ep", "tp"),
            P("ep", "tp"),
            P("ep", "tp"),
            P("tp"),
            P(None, "tp"),
            P(),
            P(),
            P("ep", None, "tp"),
            P("ep", None, "tp"),
            P("ep", None, "tp"),
            P("ep", None),
            P("ep", None),
        ),
        out_specs=(P("ep", "tp"), P("ep", "tp", None, None)),
        check_vma=False,
    )
```

```python
import functools

import jax
import jax.numpy as jnp
import numpy as np
from jax import lax
from jax.experimental import pallas as pl
from jax.experimental.pallas import tpu as pltpu
from jax.sharding import PartitionSpec as P

MESH = pl.DeviceIdType.MESH
F32 = jnp.float32
BF16 = jnp.bfloat16
D = 4096
RD = 2048
HEADS = 16
HEAD = 128
ROWS = 40
COLS = 256
NEP = 16
NTP = 16
NZ = 8
SLOTS = 128
GROUPS_OF_ROWS = ROWS // 8
EPS = 1e-06


def constants():
    table = np.zeros((24, 128), np.float64)
    heads = np.arange(HEADS, dtype=np.float64)
    table[:HEADS] = (1.0 - 2.0 ** (-5.0 - 5.0 * heads / (HEADS - 1)))[:, None]
    inverse = 10000.0 ** (-np.arange(0, HEAD, 2, dtype=np.float64) / HEAD)
    table[HEADS] = np.concatenate([inverse, inverse])
    return table.astype(np.float32)


TRACE = False
_open = []


def mark(name):
    if not TRACE:
        return
    while _open:
        _open.pop().__exit__(None, None, None)
    if name:
        _open.append(jax.named_scope(name))
        _open[-1].__enter__()


def ring_offset(i):
    half = i // 2 + 1
    return half + (i % 2) * (NZ - 2 * half)


def body(
    hidden,
    positions,
    ret_state,
    query_weight,
    key_weight,
    value_weight,
    gate_weight,
    head_gain,
    out_weight,
    mix_gain,
    ffn_gain,
    expert_gate,
    expert_up,
    expert_down,
    route_ids,
    route_weight,
    table,
    updated,
    state_parts,
    v_hidden,
    v_pos,
    v_state,
    v_qkvg,
    v_head_gain,
    v_out,
    v_mix_gain,
    v_ffn_gain,
    v_gu,
    v_down,
    v_ids,
    v_weight,
    v_table,
    agbuf,
    xbuf,
    bacc,
    bsend,
    brecv,
    ssout,
    ssin,
    readbuf,
    cbuf,
    afters,
    psend,
    dbuf,
    acc_gu,
    ebuf,
    acc_down,
    fsend,
    frecv,
    local_sem,
    w_send,
    w_recv,
    a1_send,
    a1_recv,
    a2_send,
    a2_recv,
    ss_sem,
    b_send,
    b_recv,
    c_send,
    c_fwd,
    c_recv,
    g_send,
    g_recv,
    d_send,
    d_fwd,
    d_recv,
    d_other,
    e_send,
    e_fwd,
    e_recv,
    f_send,
    f_recv,
):
    ep = lax.axis_index("ep")
    tp = lax.axis_index("tp")
    z = tp // 2
    core = tp % 2
    other = 2 * z + 1 - core
    down = ep // 4
    across = ep % 4

    mark("load")
    loads = [
        (hidden, v_hidden),
        (positions, v_pos),
        (table, v_table),
        (route_ids, v_ids),
        (route_weight, v_weight),
        (head_gain, v_head_gain),
        (mix_gain, v_mix_gain),
        (ffn_gain, v_ffn_gain),
        (query_weight, v_qkvg.at[across, :, pl.ds(0, 128)]),
        (key_weight, v_qkvg.at[across, :, pl.ds(128, 128)]),
        (value_weight, v_qkvg.at[across, :, pl.ds(256, 128)]),
        (gate_weight, v_qkvg.at[across, :, pl.ds(384, 128)]),
        (ret_state, v_state),
        (out_weight, v_out),
        (expert_gate, v_gu.at[:, :, pl.ds(0, 128)]),
        (expert_up, v_gu.at[:, :, pl.ds(128, 128)]),
        (expert_down, v_down),
    ]
    copies = [pltpu.make_async_copy(src, dst, local_sem.at[i]) for i, (src, dst) in enumerate(loads)]
    for copy in copies[:12]:
        copy.start()

    barrier = pltpu.get_barrier_semaphore()

    def greet_plane(i, carry):
        peer = (ep + i) % NEP
        pl.semaphore_signal(barrier, inc=1, device_id=(peer, tp), device_id_type=MESH)
        pl.semaphore_signal(barrier, inc=1, device_id=(peer, other), device_id_type=MESH)
        return carry

    def greet_ring(i, carry):
        peer = 2 * ((z + i) % NZ) + core
        pl.semaphore_signal(barrier, inc=1, device_id=(ep, peer), device_id_type=MESH)
        return carry

    lax.fori_loop(1, NEP, greet_plane, 0)
    lax.fori_loop(1, NZ, greet_ring, 0)
    pl.semaphore_signal(barrier, inc=1, device_id=(ep, other), device_id_type=MESH)
    for copy in copies[12:]:
        copy.start()
    for copy in copies[:8]:
        copy.wait()
    agbuf[pl.ds(z, 1)] = v_hidden[...].reshape(1, ROWS, COLS)

    mark("prep")
    token = lax.broadcasted_iota(jnp.int32, (ROWS, ROWS), 0)
    other_token = lax.broadcasted_iota(jnp.int32, (ROWS, ROWS), 1)

    def column(row):
        return jnp.sum(jnp.where(token == other_token, row.astype(F32), 0.0), axis=1, keepdims=True)

    inverse = v_table[HEADS : HEADS + 1, :]
    angle = column(v_pos[...]) * inverse
    cosine = jnp.cos(angle)
    sine = jnp.sin(angle)
    lane = lax.broadcasted_iota(jnp.int32, (ROWS, 128), 1)
    sine = jnp.where(lane < HEAD // 2, -sine, sine)

    slot_expert = lane // 4
    slot_expert = slot_expert.astype(F32)
    first = column(v_ids[0:1, :]) == slot_expert
    second = column(v_ids[1:2, :]) == slot_expert
    named = jnp.where(first | second, 1.0, 0.0).astype(F32)
    earlier = jnp.where(token > other_token, 1.0, 0.0).astype(BF16)
    ranks = jnp.dot(earlier, named.astype(BF16), preferred_element_type=F32)
    placed = jnp.where(ranks == (lane % 4).astype(F32), named, 0.0)
    combine = placed * jnp.where(first, column(v_weight[0:1, :]), column(v_weight[1:2, :]))

    mark("barrier")
    pl.semaphore_wait(barrier, 2 * (NEP - 1) + (NZ - 1) + 1)

    def copy_to(src, dst, send_sem, recv_sem, to_ep, to_tp):
        return pltpu.make_async_remote_copy(
            src_ref=src,
            dst_ref=dst,
            send_sem=send_sem,
            recv_sem=recv_sem,
            device_id=(to_ep, to_tp),
            device_id_type=MESH,
        )

    right = 4 * down + (across + 1) % 4
    left = 4 * down + (across + 3) % 4

    def w_copy(block, half, way, i):
        part = v_qkvg.at[block, pl.ds(half * 128, 128)]
        return copy_to(
            part, part, w_send.at[way, i], w_recv.at[block, half], right if way == 0 else left, tp
        )

    for copy in copies[8:12]:
        copy.wait()
    w_sends = [
        w_copy(across, 0, 0, 0),
        w_copy(across, 1, 1, 0),
        w_copy(across, 1, 0, 1),
        w_copy(across, 0, 1, 1),
        w_copy(left % 4, 0, 0, 2),
        w_copy(right % 4, 1, 1, 2),
    ]

    def a1_copy(i, slot):
        peer = 2 * ((z + ring_offset(i)) % NZ) + core
        return copy_to(v_hidden, agbuf.at[slot], a1_send.at[i], a1_recv.at[slot], ep, peer)

    def a1_start(i, carry):
        a1_copy(NZ - 2 - i, z).start()
        return carry

    lax.fori_loop(0, NZ - 1, a1_start, 0)
    for copy in w_sends[:4]:
        copy.start()

    def near(i):
        return i + (i // 2) * (5 - 2 * i)

    def a2_copy(row, cc):
        return copy_to(
            agbuf.at[pl.ds(2 * row, 2)],
            xbuf.at[down, core],
            a2_send.at[row, cc],
            a2_recv.at[down, core],
            4 * row + across,
            2 * z + cc,
        )

    def a2_start(i, carry):
        row = (z // 2 + near(i)) % 4
        for k in range(2):
            slot = 2 * row + k

            @pl.when(slot != z)
            def _():
                a1_copy(0, slot).wait_recv()

        for cc in range(2):
            mine = (row == down) & (cc == core)

            @pl.when(jnp.logical_not(mine))
            def _():
                a2_copy(row, cc).start()

            @pl.when(mine)
            def _():
                xbuf[pl.ds(row, 1), pl.ds(core, 1)] = agbuf[pl.ds(2 * row, 2)].reshape(
                    1, 1, 2, ROWS, COLS
                )

        return carry

    mark("a1_wait_a2_issue")
    lax.fori_loop(0, 4, a2_start, 0)
    mark("w_forward")
    w_copy(left % 4, 0, 0, 0).wait_recv()
    w_sends[4].start()
    w_copy(right % 4, 1, 1, 0).wait_recv()
    w_sends[5].start()

    mark("ss")
    def square(i, total):
        part = agbuf[pl.ds(i, 1)].reshape(ROWS, COLS).astype(F32)
        part = part * part
        return total + part[:, :128] + part[:, 128:]

    ssout[...] = lax.fori_loop(0, NZ, square, jnp.zeros((ROWS, 128), F32))
    ss_copy = copy_to(ssout, ssin, ss_sem.at[0], ss_sem.at[1], ep, other)
    ss_copy.start()

    def plane_peer(i):
        down, along = i // 4, i % 4
        down = down + (down // 2) * (5 - 2 * down)
        along = along + (along // 2) * (5 - 2 * along)
        return ((ep // 4 + down) % 4) * 4 + (ep + along) % 4

    def b_copy(slot, row):
        return copy_to(
            bsend.at[row], brecv.at[slot], b_send.at[row], b_recv.at[slot], 4 * row + across, tp
        )

    mark("a2_wait")
    for row in range(4):
        for parity in range(2):

            @pl.when((row != down) | (parity != core))
            def _():
                block = xbuf.at[row, parity]
                copy_to(block, block, a2_send.at[0, 0], a2_recv.at[row, parity], ep, other).wait_recv()

    def partial(block):
        at = pl.multiple_of((4 * down + block) * COLS, COLS)
        gain = v_mix_gain[:, pl.ds(at, COLS)].reshape(1, 1, COLS)
        rows = xbuf[:, pl.ds(block % 2, 1), pl.ds(block // 2, 1)].reshape(4, ROWS, COLS)
        rows = (rows.astype(F32) * gain).reshape(4 * ROWS, COLS).astype(BF16)
        return jnp.dot(
            rows, v_qkvg[pl.ds(block, 1)].reshape(COLS, 512), preferred_element_type=F32
        )

    mark("b_rows")
    bacc[...] = partial(across)
    w_copy(left % 4, 1, 0, 0).wait_recv()
    bacc[...] += partial(left % 4)
    w_copy(right % 4, 0, 1, 0).wait_recv()
    bacc[...] += partial(right % 4)
    opposite = (across + 2) % 4
    mark("w_wait")
    w_copy(opposite, 0, 0, 0).wait_recv()
    w_copy(opposite, 1, 1, 0).wait_recv()
    mark("b_last")
    bsend[...] = (bacc[...] + partial(opposite)).reshape(4, ROWS, 512).astype(BF16)

    def b_start(i, carry):
        b_copy(down, (down + near(3 - i)) % 4).start()
        return carry

    lax.fori_loop(0, 3, b_start, 0)
    brecv[pl.ds(down, 1)] = bsend[pl.ds(down, 1)]

    mark("ss_wait")
    ss_copy.wait_recv()
    square_sum = jnp.sum(ssout[...] + ssin[...], axis=-1, keepdims=True)
    factor = lax.rsqrt(square_sum * (1.0 / D) + EPS)

    mark("b_sum")

    def b_wait(i, carry):
        row = (down + near(i)) % 4
        b_copy(row, row).wait_recv()
        return carry

    lax.fori_loop(1, 4, b_wait, 0)
    part = brecv[...].astype(F32)
    joined = (part[0] + part[1]) + (part[2] + part[3])
    joined = (joined * factor).astype(BF16).astype(F32)

    mark("rot")
    def rotate(values):
        return values * cosine + pltpu.roll(values, HEAD // 2, 1) * sine

    rotated_query = rotate(joined[:, :128])
    rotated_key = rotate(joined[:, 128:256]) * HEAD ** (-0.5)
    value = joined[:, 256:384]
    gate_rows = joined[:, 384:]
    decay = v_table[pl.ds(tp, 1), :]
    readbuf[0] = rotated_query
    readbuf[1] = rotated_key
    readbuf[2] = value
    state_parts[0] = rotated_key
    state_parts[1] = value
    mark("retain")
    copies[12].wait()

    def retain(group, carry):
        at = pl.ds(pl.multiple_of(8 * group, 8), 8)
        query_columns = readbuf[0, at, :].T
        key_columns = readbuf[1, at, :].T
        values = readbuf[2, at, :]
        reads = []
        for k in range(8):
            state = (
                decay * v_state[8 * group + k, 0] + key_columns[:, k : k + 1] * values[k : k + 1, :]
            )
            reads.append(jnp.sum(query_columns[:, k : k + 1] * state, axis=0, keepdims=True))
        readbuf[3, at, :] = jnp.concatenate(reads, axis=0)
        return carry

    lax.fori_loop(0, ROWS // 8, retain, 0)
    mark("groupnorm")
    read = readbuf[3]
    centered = read - jnp.mean(read, axis=-1, keepdims=True)
    normal = centered * lax.rsqrt(jnp.mean(centered * centered, axis=-1, keepdims=True) + EPS)
    mixed = normal * v_head_gain[...] * jax.nn.silu(gate_rows)
    cbuf[pl.ds(tp, 1)] = mixed.astype(BF16).reshape(1, ROWS, HEAD)

    def gather(buf, send_sem, fwd_sem, recv_sem, consume):
        def direct(i, slot):
            peer = 2 * ((z + ring_offset(i)) % NZ) + core
            return copy_to(buf.at[slot], buf.at[slot], send_sem.at[i], recv_sem.at[slot], ep, peer)

        def forward(row, slot):
            return copy_to(
                buf.at[slot], buf.at[slot], fwd_sem.at[row], recv_sem.at[slot], ep, other
            )

        def begin(i, carry):
            direct(NZ - 2 - i, tp).start()
            return carry

        lax.fori_loop(0, NZ - 1, begin, 0)
        forward(z, tp).start()

        def step(i, carry):
            @pl.when(i < NZ - 1)
            def _():
                row = (z + ring_offset(i)) % NZ
                direct(0, 2 * row + core).wait_recv()
                forward(row, 2 * row + core).start()

            before = lax.select(i > 0, (z + ring_offset(lax.max(i - 1, 0))) % NZ, z)
            forward(before, 2 * before + 1 - core).wait_recv()
            consume(before, i == 0)
            return carry

        lax.fori_loop(0, NZ, step, 0)

        def finish():
            def one(i, carry):
                direct(i, tp).wait_send()
                forward((z + ring_offset(i)) % NZ, tp).wait_send()
                return carry

            lax.fori_loop(0, NZ - 1, one, 0)
            forward(z, tp).wait_send()

        return finish

    copies[13].wait()
    projected = readbuf.at[pl.ds(0, 2)]

    def project(row, first_step):
        pair = cbuf[pl.ds(2 * row, 2)].astype(F32)
        block = jnp.concatenate([pair[0], pair[1]], axis=1).astype(BF16)
        part = jnp.dot(
            block,
            v_out[pl.ds(pl.multiple_of(row * COLS, COLS), COLS), :],
            preferred_element_type=F32,
        )

        @pl.when(first_step)
        def _():
            projected[0] = part[:, :128]
            projected[1] = part[:, 128:]

        @pl.when(jnp.logical_not(first_step))
        def _():
            projected[0] += part[:, :128]
            projected[1] += part[:, 128:]

    mark("c_gather")
    finish_c = gather(cbuf, c_send, c_fwd, c_recv, project)
    mark("after_pack")
    own = v_hidden[...].astype(F32)
    after = (own + jnp.concatenate([projected[0], projected[1]], axis=1)).astype(BF16)
    afters[pl.ds(z, 1)] = after.reshape(1, ROWS, COLS)

    def g_copy(i, slot):
        peer = 2 * ((z + ring_offset(i)) % NZ) + core
        return copy_to(afters.at[z], afters.at[slot], g_send.at[i], g_recv.at[slot], ep, peer)

    def g_start(i, carry):
        g_copy(NZ - 2 - i, z).start()
        return carry

    lax.fori_loop(0, NZ - 1, g_start, 0)

    def halves_below(array):
        parts = [array[:, :128].reshape(NEP, 8, 128), array[:, 128:].reshape(NEP, 8, 128)]
        return jnp.concatenate(parts, axis=1)

    def halves_beside(array):
        array = array.astype(F32)
        return array[:, :8].reshape(SLOTS, 128), array[:, 8:].reshape(SLOTS, 128)

    placing = placed.astype(BF16)

    def pack(row):
        packed = lax.dot_general(
            placing,
            afters[pl.ds(row, 1)].reshape(ROWS, COLS),
            (((0,), (0,)), ((), ())),
            preferred_element_type=F32,
        )
        psend[:, pl.ds(row, 1)] = halves_below(packed).astype(BF16).reshape(NEP, 1, 16, 128)

    pack(z)

    def pack_next(i, carry):
        row = (z + ring_offset(i)) % NZ
        g_copy(i, row).wait_recv()
        pack(row)
        return carry

    mark("after_gather")
    lax.fori_loop(0, NZ - 1, pack_next, 0)

    def d_copy(peer, source):
        return copy_to(
            psend.at[peer], dbuf.at[core, source], d_send.at[peer], d_recv.at[source], peer, tp
        )

    def d_forward(parity, source):
        block = dbuf.at[parity, source]
        return copy_to(block, block, d_fwd.at[source], d_other.at[source], ep, other)

    def d_start(i, carry):
        d_copy(plane_peer(NEP - 1 - i), ep).start()
        return carry

    mark("d_issue")
    lax.fori_loop(0, NEP - 1, d_start, 0)
    dbuf[pl.ds(core, 1), pl.ds(ep, 1)] = psend[pl.ds(ep, 1)].reshape(1, 1, NZ, 16, 128)
    d_forward(core, ep).start()

    def d_arrive(i, carry):
        peer = plane_peer(i)
        d_copy(peer, peer).wait_recv()
        d_forward(core, peer).start()
        return carry

    acc_gu[...] = jnp.zeros_like(acc_gu)
    mark("d_wait")
    lax.fori_loop(1, NEP, d_arrive, 0)
    copies[14].wait()
    copies[15].wait()
    square_of = acc_gu.at[2]

    def lift(parity):
        def one(row, carry):
            at = pl.multiple_of((2 * row + parity) * COLS, COLS)
            block = dbuf[pl.ds(parity, 1), :, pl.ds(row, 1)].reshape(NEP, 16, 128)
            low, high = halves_beside(block)
            square_of[:, :128] += low * low + high * high
            both = jnp.concatenate([low, high], axis=1) * v_ffn_gain[:, pl.ds(at, COLS)]
            both = both.astype(BF16)
            for j in range(2):
                acc_gu[j] += jnp.dot(both, v_gu[j, pl.ds(at, COLS), :], preferred_element_type=F32)
            return carry

        lax.fori_loop(0, NZ, one, 0)

    mark("lift_own")
    lift(core)

    def d_other_wait(source, carry):
        d_forward(1 - core, source).wait_recv()
        return carry

    mark("lift_wait")
    lax.fori_loop(0, NEP, d_other_wait, 0)
    mark("lift_other")
    lift(1 - core)
    mark("act")
    inner = lax.rsqrt(
        jnp.sum(square_of[:, :128], axis=-1, keepdims=True) * (1.0 / D) + EPS
    )
    own_expert = lax.broadcasted_iota(jnp.int32, (SLOTS, COLS), 0) % 8 < 4
    chosen = jnp.where(own_expert, acc_gu[0], acc_gu[1]) * inner
    activated = jax.nn.silu(chosen[:, :128]) * chosen[:, 128:]
    ebuf[pl.ds(tp, 1)] = activated.astype(BF16).reshape(1, SLOTS, 128)
    copies[16].wait()

    def lower(row, first_step):
        @pl.when(first_step)
        def _():
            acc_down[...] = jnp.zeros_like(acc_down)

        pair = ebuf[pl.ds(2 * row, 2)]
        both = jnp.concatenate([pair[0], pair[1]], axis=1)
        at = pl.multiple_of(row * COLS, COLS)
        for j in range(2):
            acc_down[j] += jnp.dot(both, v_down[j, pl.ds(at, COLS), :], preferred_element_type=F32)

    mark("e_gather")
    finish_e = gather(ebuf, e_send, e_fwd, e_recv, lower)
    mark("result")
    result = jnp.where(own_expert, acc_down[0], acc_down[1])

    fsend[...] = halves_below(result).astype(BF16)

    def f_copy(peer, source):
        return copy_to(
            fsend.at[peer], frecv.at[source], f_send.at[peer], f_recv.at[source], peer, tp
        )

    def f_start(i, carry):
        f_copy((ep + i) % NEP, ep).start()
        return carry

    lax.fori_loop(1, NEP, f_start, 0)
    frecv[pl.ds(ep, 1)] = fsend[pl.ds(ep, 1)]

    mark("sent")
    def sent_ring(i, carry):
        a1_copy(i, z).wait_send()
        g_copy(i, z).wait_send()
        return carry

    lax.fori_loop(0, NZ - 1, sent_ring, 0)

    for row in range(4):
        for cc in range(2):

            @pl.when((row != down) | (cc != core))
            def _():
                a2_copy(row, cc).wait_send()

    for copy in w_sends:
        copy.wait_send()

    def sent_b(i, carry):
        b_copy(down, (down + near(i)) % 4).wait_send()
        return carry

    lax.fori_loop(1, 4, sent_b, 0)
    ss_copy.wait_send()
    d_forward(core, ep).wait_send()

    def sent_plane(i, carry):
        peer = (ep + i) % NEP
        d_copy(peer, ep).wait_send()
        d_forward(core, peer).wait_send()
        return carry

    lax.fori_loop(1, NEP, sent_plane, 0)
    finish_c()
    finish_e()

    def f_wait(i, carry):
        peer = (ep + i) % NEP
        f_copy(peer, peer).wait_recv()
        return carry

    mark("f_wait")
    lax.fori_loop(1, NEP, f_wait, 0)
    mark("combine")
    back = jnp.concatenate(halves_beside(frecv[...]), axis=1)
    weighted = jnp.dot(
        combine, back, preferred_element_type=F32, precision=lax.Precision.HIGHEST
    )
    updated[...] = (after.astype(F32) + weighted).astype(BF16)

    def f_sent(i, carry):
        f_copy((ep + i) % NEP, ep).wait_send()
        return carry

    lax.fori_loop(1, NEP, f_sent, 0)
    mark("")


def state_body(
    before, parts, table, ret_state, updated, next_state, v_updated, v_parts, v_table, v_state, sem, load, store
):
    copies = [
        pltpu.make_async_copy(parts, v_parts, sem.at[0]),
        pltpu.make_async_copy(table, v_table, sem.at[1]),
        pltpu.make_async_copy(before, v_updated, sem.at[2]),
    ]
    out = pltpu.make_async_copy(v_updated, updated, sem.at[3])

    def rows_in(group):
        at = pl.ds(8 * group, 8)
        return pltpu.make_async_copy(ret_state.at[at], v_state.at[at], load.at[group])

    def rows_out(group):
        at = pl.ds(8 * group, 8)
        return pltpu.make_async_copy(v_state.at[at], next_state.at[at], store.at[group])

    for copy in copies:
        copy.start()
    for group in range(GROUPS_OF_ROWS):
        rows_in(group).start()
    for copy in copies:
        copy.wait()
    out.start()
    decay = v_table[pl.ds(lax.axis_index("tp"), 1), :]

    def one(group, carry):
        at = pl.ds(pl.multiple_of(8 * group, 8), 8)
        key_columns = v_parts[0, at, :].T
        values = v_parts[1, at, :]
        rows_in(group).wait()
        for k in range(8):
            v_state[8 * group + k, 0] = (
                decay * v_state[8 * group + k, 0] + key_columns[:, k : k + 1] * values[k : k + 1, :]
            )
        rows_out(group).start()
        return carry

    lax.fori_loop(0, GROUPS_OF_ROWS, one, 0)
    out.wait()
    for group in range(GROUPS_OF_ROWS):
        rows_out(group).wait()


def per_device(
    hidden,
    positions,
    ret_state,
    query_weight,
    key_weight,
    value_weight,
    gate_weight,
    head_gain,
    out_weight,
    mix_gain,
    ffn_gain,
    expert_gate,
    expert_up,
    expert_down,
    route_ids,
    route_weight,
):
    table = jnp.asarray(constants())
    dma = pltpu.SemaphoreType.DMA
    vmem = pltpu.VMEM
    anywhere = pl.BlockSpec(memory_space=pltpu.HBM)
    updated, parts = pl.pallas_call(
        body,
        out_shape=(
            jax.ShapeDtypeStruct((ROWS, COLS), BF16),
            jax.ShapeDtypeStruct((2, ROWS, HEAD), F32),
        ),
        in_specs=[anywhere] * 17,
        out_specs=(pl.BlockSpec(memory_space=pltpu.VMEM),) * 2,
        scratch_shapes=[
            vmem((ROWS, COLS), BF16),
            vmem((1, ROWS), jnp.int32),
            vmem((ROWS, 1, HEAD, HEAD), F32),
            vmem((4, COLS, 512), BF16),
            vmem((1, HEAD), F32),
            vmem((RD, COLS), BF16),
            vmem((1, D), F32),
            vmem((1, D), F32),
            vmem((2, D, COLS), BF16),
            vmem((2, RD, COLS), BF16),
            vmem((2, ROWS), jnp.int32),
            vmem((2, ROWS), F32),
            vmem((24, 128), F32),
            vmem((NZ, ROWS, COLS), BF16),
            vmem((4, 2, 2, ROWS, COLS), BF16),
            vmem((4 * ROWS, 512), F32),
            vmem((4, ROWS, 512), BF16),
            vmem((4, ROWS, 512), BF16),
            vmem((ROWS, 128), F32),
            vmem((ROWS, 128), F32),
            vmem((4, ROWS, HEAD), F32),
            vmem((NTP, ROWS, HEAD), BF16),
            vmem((NZ, ROWS, COLS), BF16),
            vmem((NEP, NZ, 16, 128), BF16),
            vmem((2, NEP, NZ, 16, 128), BF16),
            vmem((3, SLOTS, COLS), F32),
            vmem((NTP, SLOTS, 128), BF16),
            vmem((2, SLOTS, COLS), F32),
            vmem((NEP, 16, 128), BF16),
            vmem((NEP, 16, 128), BF16),
            dma((17,)),
            dma((2, 3)),
            dma((4, 2)),
            dma((NZ,)),
            dma((NZ,)),
            dma((4, 2)),
            dma((4, 2)),
            dma((2,)),
            dma((4,)),
            dma((4,)),
            dma((NZ,)),
            dma((NZ,)),
            dma((NTP,)),
            dma((NZ,)),
            dma((NZ,)),
            dma((NEP,)),
            dma((NEP,)),
            dma((NEP,)),
            dma((NEP,)),
            dma((NZ,)),
            dma((NZ,)),
            dma((NTP,)),
            dma((NEP,)),
            dma((NEP,)),
        ],
        compiler_params=pltpu.CompilerParams(
            collective_id=0, has_side_effects=True, vmem_limit_bytes=67043328
        ),
    )(
        hidden,
        positions.reshape(1, ROWS),
        ret_state,
        query_weight,
        key_weight,
        value_weight,
        gate_weight,
        head_gain.reshape(1, HEAD),
        out_weight,
        mix_gain.reshape(1, D),
        ffn_gain.reshape(1, D),
        expert_gate,
        expert_up,
        expert_down,
        route_ids.T,
        route_weight.T,
        table,
    )
    return pl.pallas_call(
        state_body,
        out_shape=(
            jax.ShapeDtypeStruct((ROWS, COLS), BF16),
            jax.ShapeDtypeStruct(ret_state.shape, F32),
        ),
        in_specs=[anywhere] * 4,
        out_specs=(anywhere,) * 2,
        scratch_shapes=[
            vmem((ROWS, COLS), BF16),
            vmem((2, ROWS, HEAD), F32),
            vmem((24, 128), F32),
            vmem((ROWS, 1, HEAD, HEAD), F32),
            dma((4,)),
            dma((GROUPS_OF_ROWS,)),
            dma((GROUPS_OF_ROWS,)),
        ],
        compiler_params=pltpu.CompilerParams(vmem_limit_bytes=67043328),
    )(updated, parts, table, ret_state)


def solution(mesh):
    return jax.shard_map(
        per_device,
        mesh=mesh,
        in_specs=(
            P("ep", "tp"),
            P("ep"),
            P("ep", "tp", None, None),
            P("ep", "tp"),
            P("ep", "tp"),
            P("ep", "tp"),
            P("ep", "tp"),
            P("tp"),
            P(None, "tp"),
            P(),
            P(),
            P("ep", None, "tp"),
            P("ep", None, "tp"),
            P("ep", None, "tp"),
            P("ep", None),
            P("ep", None),
        ),
        out_specs=(P("ep", "tp"), P("ep", "tp", None, None)),
        check_vma=False,
    )
```

```python
import functools

import jax
import jax.numpy as jnp
import numpy as np
from jax import lax
from jax.experimental import pallas as pl
from jax.experimental.pallas import tpu as pltpu
from jax.sharding import PartitionSpec as P

MESH = pl.DeviceIdType.MESH
F32 = jnp.float32
BF16 = jnp.bfloat16
D = 4096
RD = 2048
HEADS = 16
HEAD = 128
ROWS = 40
COLS = 256
NEP = 16
NTP = 16
NZ = 8
SLOTS = 128
LIMIT = 67043328 - 40 * 128 * 128 * 4 - 2 * 16384 * 2
GROUPS_OF_ROWS = ROWS // 8
EPS = 1e-06


def constants():
    table = np.zeros((24, 128), np.float64)
    heads = np.arange(HEADS, dtype=np.float64)
    table[:HEADS] = (1.0 - 2.0 ** (-5.0 - 5.0 * heads / (HEADS - 1)))[:, None]
    inverse = 10000.0 ** (-np.arange(0, HEAD, 2, dtype=np.float64) / HEAD)
    table[HEADS] = np.concatenate([inverse, inverse])
    return table.astype(np.float32)


TRACE = False
_open = []


def mark(name):
    if not TRACE:
        return
    while _open:
        _open.pop().__exit__(None, None, None)
    if name:
        _open.append(jax.named_scope(name))
        _open[-1].__enter__()


def ring_offset(i):
    half = i // 2 + 1
    return half + ((i + 1) % 2) * (NZ - 2 * half)


def body(
    hidden,
    positions,
    ret_state,
    query_weight,
    key_weight,
    value_weight,
    gate_weight,
    head_gain,
    out_weight,
    mix_gain,
    ffn_gain,
    expert_gate,
    expert_up,
    expert_down,
    route_ids,
    route_weight,
    table,
    updated,
    v_state,
    v_hidden,
    v_pos,
    v_qkvg,
    v_head_gain,
    v_out,
    v_mix_gain,
    v_ffn_gain,
    v_gu,
    v_down,
    v_ids,
    v_weight,
    v_table,
    agbuf,
    xbuf,
    bacc,
    bsend,
    brecv,
    ssout,
    ssin,
    readbuf,
    cbuf,
    afters,
    psend,
    dbuf,
    lifted,
    acc_gu,
    ebuf,
    acc_down,
    fsend,
    frecv,
    local_sem,
    gu_sem,
    w_send,
    w_recv,
    a1_send,
    a1_recv,
    a2_send,
    a2_recv,
    ss_sem,
    b_send,
    b_recv,
    c_send,
    c_fwd,
    c_recv,
    g_send,
    g_recv,
    d_send,
    d_fwd,
    d_recv,
    d_other,
    e_send,
    e_fwd,
    e_recv,
    f_send,
    f_recv,
):
    ep = lax.axis_index("ep")
    tp = lax.axis_index("tp")
    z = tp // 2
    core = tp % 2
    other = 2 * z + 1 - core
    down = ep // 4
    across = ep % 4

    mark("load")
    loads = [
        (hidden, v_hidden),
        (positions, v_pos),
        (table, v_table),
        (route_ids, v_ids),
        (route_weight, v_weight),
        (head_gain, v_head_gain),
        (mix_gain, v_mix_gain),
        (ffn_gain, v_ffn_gain),
        (query_weight, v_qkvg.at[across, :, pl.ds(0, 128)]),
        (key_weight, v_qkvg.at[across, :, pl.ds(128, 128)]),
        (value_weight, v_qkvg.at[across, :, pl.ds(256, 128)]),
        (gate_weight, v_qkvg.at[across, :, pl.ds(384, 128)]),
        (ret_state, v_state),
        (out_weight, v_out),
        (expert_down, v_down),
    ]
    copies = [pltpu.make_async_copy(src, dst, local_sem.at[i]) for i, (src, dst) in enumerate(loads)]
    for copy in copies[:12]:
        copy.start()

    def relative(i):
        return (z + (i + 1) // 2 * (1 - i % 2 * 2) + NZ) % NZ

    def lift_load(i, up):
        parity, place = i // NZ, i % NZ
        source = pl.multiple_of((2 * relative(place) + parity) * COLS, COLS)
        return pltpu.make_async_copy(
            (expert_up if up else expert_gate).at[:, pl.ds(source, COLS)],
            v_gu.at[:, pl.ds(pl.multiple_of(i * COLS, COLS), COLS), pl.ds(128 * up, 128)],
            gu_sem.at[i, up],
        )

    def lift_loads(i, carry):
        lift_load(i, 0).start()
        lift_load(i, 1).start()
        return carry

    def lift_loaded(i, carry):
        lift_load(i, 0).wait()
        lift_load(i, 1).wait()
        return carry

    barrier = pltpu.get_barrier_semaphore()

    def greet_plane(i, carry):
        peer = (ep + i) % NEP
        pl.semaphore_signal(barrier, inc=1, device_id=(peer, tp), device_id_type=MESH)
        pl.semaphore_signal(barrier, inc=1, device_id=(peer, other), device_id_type=MESH)
        return carry

    def greet_ring(i, carry):
        peer = 2 * ((z + i) % NZ) + core
        pl.semaphore_signal(barrier, inc=1, device_id=(ep, peer), device_id_type=MESH)
        return carry

    lax.fori_loop(1, NEP, greet_plane, 0)
    lax.fori_loop(1, NZ, greet_ring, 0)
    pl.semaphore_signal(barrier, inc=1, device_id=(ep, other), device_id_type=MESH)
    for copy in copies[12:]:
        copy.start()
    lax.fori_loop(0, NTP, lift_loads, 0)
    for copy in copies[:8]:
        copy.wait()
    agbuf[pl.ds(z, 1)] = v_hidden[...].reshape(1, ROWS, COLS)

    mark("prep")
    token = lax.broadcasted_iota(jnp.int32, (ROWS, ROWS), 0)
    other_token = lax.broadcasted_iota(jnp.int32, (ROWS, ROWS), 1)

    def column(row):
        return jnp.sum(jnp.where(token == other_token, row.astype(F32), 0.0), axis=1, keepdims=True)

    inverse = v_table[HEADS : HEADS + 1, :]
    angle = column(v_pos[...]) * inverse
    cosine = jnp.cos(angle)
    sine = jnp.sin(angle)
    lane = lax.broadcasted_iota(jnp.int32, (ROWS, 128), 1)
    sine = jnp.where(lane < HEAD // 2, -sine, sine)

    slot_expert = lane // 4
    slot_expert = slot_expert.astype(F32)
    first = column(v_ids[0:1, :]) == slot_expert
    second = column(v_ids[1:2, :]) == slot_expert
    named = jnp.where(first | second, 1.0, 0.0).astype(F32)
    earlier = jnp.where(token > other_token, 1.0, 0.0).astype(BF16)
    ranks = jnp.dot(earlier, named.astype(BF16), preferred_element_type=F32)
    placed = jnp.where(ranks == (lane % 4).astype(F32), named, 0.0)
    combine = placed * jnp.where(first, column(v_weight[0:1, :]), column(v_weight[1:2, :]))

    mark("barrier")
    pl.semaphore_wait(barrier, 2 * (NEP - 1) + (NZ - 1) + 1)

    def copy_to(src, dst, send_sem, recv_sem, to_ep, to_tp):
        return pltpu.make_async_remote_copy(
            src_ref=src,
            dst_ref=dst,
            send_sem=send_sem,
            recv_sem=recv_sem,
            device_id=(to_ep, to_tp),
            device_id_type=MESH,
        )

    right = 4 * down + (across + 1) % 4
    left = 4 * down + (across + 3) % 4

    def w_copy(block, half, way, i):
        part = v_qkvg.at[block, pl.ds(half * 128, 128)]
        return copy_to(
            part, part, w_send.at[way, i], w_recv.at[block, half], right if way == 0 else left, tp
        )

    for copy in copies[8:12]:
        copy.wait()
    w_sends = [
        w_copy(across, 0, 0, 0),
        w_copy(across, 1, 1, 0),
        w_copy(across, 1, 0, 1),
        w_copy(across, 0, 1, 1),
        w_copy(left % 4, 0, 0, 2),
        w_copy(right % 4, 1, 1, 2),
    ]

    def a1_copy(i, slot):
        peer = 2 * ((z + ring_offset(i)) % NZ) + core
        return copy_to(v_hidden, agbuf.at[slot], a1_send.at[i], a1_recv.at[slot], ep, peer)

    def a1_start(i, carry):
        a1_copy(NZ - 2 - i, z).start()
        return carry

    lax.fori_loop(0, NZ - 1, a1_start, 0)
    for copy in w_sends[:4]:
        copy.start()

    def near(i):
        return i + (i // 2) * (5 - 2 * i)

    def a2_copy(row, cc):
        return copy_to(
            agbuf.at[pl.ds(2 * row, 2)],
            xbuf.at[down, core],
            a2_send.at[row, cc],
            a2_recv.at[down, core],
            4 * row + across,
            2 * z + cc,
        )

    def a2_start(i, carry):
        row = (z // 2 + near(i)) % 4
        for k in range(2):
            slot = 2 * row + k

            @pl.when(slot != z)
            def _():
                a1_copy(0, slot).wait_recv()

        for cc in range(2):
            mine = (row == down) & (cc == core)

            @pl.when(jnp.logical_not(mine))
            def _():
                a2_copy(row, cc).start()

            @pl.when(mine)
            def _():
                xbuf[pl.ds(row, 1), pl.ds(core, 1)] = agbuf[pl.ds(2 * row, 2)].reshape(
                    1, 1, 2, ROWS, COLS
                )

        return carry

    mark("a1_wait_a2_issue")
    lax.fori_loop(0, 4, a2_start, 0)
    mark("w_forward")
    w_copy(left % 4, 0, 0, 0).wait_recv()
    w_sends[4].start()
    w_copy(right % 4, 1, 1, 0).wait_recv()
    w_sends[5].start()

    mark("ss")
    def square(i, total):
        part = agbuf[pl.ds(i, 1)].reshape(ROWS, COLS).astype(F32)
        part = part * part
        return total + part[:, :128] + part[:, 128:]

    ssout[...] = lax.fori_loop(0, NZ, square, jnp.zeros((ROWS, 128), F32))
    ss_copy = copy_to(ssout, ssin, ss_sem.at[0], ss_sem.at[1], ep, other)
    ss_copy.start()

    steps = (0, 1, 3, 2)
    plane = [
        4 * lax.rem(down + row, 4) + lax.rem(across + column_step, 4)
        for row in steps
        for column_step in steps
    ]

    def b_copy(slot, row):
        return copy_to(
            bsend.at[row], brecv.at[slot], b_send.at[row], b_recv.at[slot], 4 * row + across, tp
        )

    mark("a2_wait")
    for row in range(4):
        for parity in range(2):

            @pl.when((row != down) | (parity != core))
            def _():
                block = xbuf.at[row, parity]
                copy_to(block, block, a2_send.at[0, 0], a2_recv.at[row, parity], ep, other).wait_recv()

    def partial(block):
        at = pl.multiple_of((4 * down + block) * COLS, COLS)
        gain = v_mix_gain[:, pl.ds(at, COLS)].reshape(1, 1, COLS)
        rows = xbuf[:, pl.ds(block % 2, 1), pl.ds(block // 2, 1)].reshape(4, ROWS, COLS)
        rows = (rows.astype(F32) * gain).reshape(4 * ROWS, COLS).astype(BF16)
        return jnp.dot(
            rows, v_qkvg[pl.ds(block, 1)].reshape(COLS, 512), preferred_element_type=F32
        )

    mark("b_rows")
    bacc[...] = partial(across)
    w_copy(left % 4, 1, 0, 0).wait_recv()
    bacc[...] += partial(left % 4)
    w_copy(right % 4, 0, 1, 0).wait_recv()
    bacc[...] += partial(right % 4)
    opposite = (across + 2) % 4
    mark("w_wait")
    w_copy(opposite, 0, 0, 0).wait_recv()
    w_copy(opposite, 1, 1, 0).wait_recv()
    mark("b_last")
    bsend[...] = (bacc[...] + partial(opposite)).reshape(4, ROWS, 512).astype(BF16)

    def b_start(i, carry):
        b_copy(down, (down + near(3 - i)) % 4).start()
        return carry

    lax.fori_loop(0, 3, b_start, 0)
    brecv[pl.ds(down, 1)] = bsend[pl.ds(down, 1)]

    mark("ss_wait")
    ss_copy.wait_recv()
    square_sum = jnp.sum(ssout[...] + ssin[...], axis=-1, keepdims=True)
    factor = lax.rsqrt(square_sum * (1.0 / D) + EPS)

    mark("b_sum")

    def b_wait(i, carry):
        row = (down + near(i)) % 4
        b_copy(row, row).wait_recv()
        return carry

    lax.fori_loop(1, 4, b_wait, 0)
    part = brecv[...].astype(F32)
    joined = (part[0] + part[1]) + (part[2] + part[3])
    joined = (joined * factor).astype(BF16).astype(F32)

    mark("rot")
    def rotate(values):
        return values * cosine + pltpu.roll(values, HEAD // 2, 1) * sine

    rotated_query = rotate(joined[:, :128])
    rotated_key = rotate(joined[:, 128:256]) * HEAD ** (-0.5)
    value = joined[:, 256:384]
    gate_rows = joined[:, 384:]
    decay = v_table[pl.ds(tp, 1), :]
    readbuf[0] = rotated_query
    readbuf[1] = rotated_key
    readbuf[2] = value
    mark("retain")
    copies[12].wait()

    def retain(group, carry):
        at = pl.ds(pl.multiple_of(8 * group, 8), 8)
        query_columns = readbuf[0, at, :].T
        key_columns = readbuf[1, at, :].T
        values = readbuf[2, at, :]
        reads = []
        for k in range(8):
            state = (
                decay * v_state[8 * group + k, 0] + key_columns[:, k : k + 1] * values[k : k + 1, :]
            )
            v_state[8 * group + k, 0] = state
            reads.append(jnp.sum(query_columns[:, k : k + 1] * state, axis=0, keepdims=True))
        readbuf[3, at, :] = jnp.concatenate(reads, axis=0)
        return carry

    lax.fori_loop(0, ROWS // 8, retain, 0)
    mark("groupnorm")
    read = readbuf[3]
    centered = read - jnp.mean(read, axis=-1, keepdims=True)
    normal = centered * lax.rsqrt(jnp.mean(centered * centered, axis=-1, keepdims=True) + EPS)
    mixed = normal * v_head_gain[...] * jax.nn.silu(gate_rows)
    cbuf[pl.ds(tp, 1)] = mixed.astype(BF16).reshape(1, ROWS, HEAD)

    def gather(buf, send_sem, fwd_sem, recv_sem, consume):
        def direct(i, slot):
            peer = 2 * ((z + ring_offset(i)) % NZ) + core
            return copy_to(buf.at[slot], buf.at[slot], send_sem.at[i], recv_sem.at[slot], ep, peer)

        def forward(row, slot):
            return copy_to(
                buf.at[slot], buf.at[slot], fwd_sem.at[row], recv_sem.at[slot], ep, other
            )

        def begin(i, carry):
            direct(i, tp).start()
            return carry

        lax.fori_loop(0, NZ - 1, begin, 0)
        forward(z, tp).start()

        def step(i, carry):
            @pl.when(i < NZ - 1)
            def _():
                row = (z + ring_offset(i)) % NZ
                direct(0, 2 * row + core).wait_recv()
                forward(row, 2 * row + core).start()

            before = lax.select(i > 0, (z + ring_offset(lax.max(i - 1, 0))) % NZ, z)
            forward(before, 2 * before + 1 - core).wait_recv()
            consume(before, i == 0)
            return carry

        lax.fori_loop(0, NZ, step, 0)

        def finish():
            def one(i, carry):
                direct(i, tp).wait_send()
                forward((z + ring_offset(i)) % NZ, tp).wait_send()
                return carry

            lax.fori_loop(0, NZ - 1, one, 0)
            forward(z, tp).wait_send()

        return finish

    copies[13].wait()
    projected = readbuf.at[pl.ds(0, 2)]

    def project(row, first_step):
        pair = cbuf[pl.ds(2 * row, 2)].astype(F32)
        block = jnp.concatenate([pair[0], pair[1]], axis=1).astype(BF16)
        part = jnp.dot(
            block,
            v_out[pl.ds(pl.multiple_of(row * COLS, COLS), COLS), :],
            preferred_element_type=F32,
        )

        @pl.when(first_step)
        def _():
            projected[0] = part[:, :128]
            projected[1] = part[:, 128:]

        @pl.when(jnp.logical_not(first_step))
        def _():
            projected[0] += part[:, :128]
            projected[1] += part[:, 128:]

    mark("c_gather")
    finish_c = gather(cbuf, c_send, c_fwd, c_recv, project)
    mark("after_pack")
    own = v_hidden[...].astype(F32)
    after = (own + jnp.concatenate([projected[0], projected[1]], axis=1)).astype(BF16)
    afters[pl.ds(z, 1)] = after.reshape(1, ROWS, COLS)

    def g_copy(i, slot):
        peer = 2 * ((z + ring_offset(i)) % NZ) + core
        return copy_to(afters.at[z], afters.at[slot], g_send.at[i], g_recv.at[slot], ep, peer)

    def g_start(i, carry):
        g_copy(i, z).start()
        return carry

    lax.fori_loop(0, NZ - 1, g_start, 0)

    def halves_below(array):
        parts = [array[:, :128].reshape(NEP, 8, 128), array[:, 128:].reshape(NEP, 8, 128)]
        return jnp.concatenate(parts, axis=1)

    def halves_beside(array):
        array = array.astype(F32)
        return array[:, :8].reshape(SLOTS, 128), array[:, 8:].reshape(SLOTS, 128)

    placing = placed.astype(BF16)

    def pack(half, k):
        packed = lax.dot_general(
            placing,
            afters[pl.ds(relative(4 * half + k), 1)].reshape(ROWS, COLS),
            (((0,), (0,)), ((), ())),
            preferred_element_type=F32,
        )
        packed = halves_below(packed).astype(BF16)
        psend[half, :, pl.ds(k, 1)] = packed.reshape(NEP, 1, 16, 128)

    def d_copy(half, peer, source):
        return copy_to(
            psend.at[half, peer],
            dbuf.at[core, half, source],
            d_send.at[half, peer],
            d_recv.at[half, source],
            peer,
            tp,
        )

    def d_forward(half, parity, source):
        block = dbuf.at[parity, half, source]
        return copy_to(block, block, d_fwd.at[half, source], d_other.at[half, source], ep, other)

    def pack_next(half):
        def one(k, carry):
            g_copy(4 * half + k - 1, relative(4 * half + k)).wait_recv()
            pack(half, k)
            return carry

        return one

    pack(0, 0)
    acc_gu[...] = jnp.zeros_like(acc_gu)
    for half in range(2):
        mark(f"after_gather{half}")
        lax.fori_loop(1 - half, 4, pack_next(half), 0)
        mark(f"d_issue{half}")
        for peer in plane[:0:-1]:
            d_copy(half, peer, ep).start()
        dbuf[pl.ds(core, 1), half, pl.ds(ep, 1)] = psend[half, pl.ds(ep, 1)].reshape(
            1, 1, 4, 16, 128
        )
        d_forward(half, core, ep).start()

    def d_arrive(half):
        for peer in plane[1:]:
            d_copy(half, peer, peer).wait_recv()
            d_forward(half, core, peer).start()

    def d_other_wait(half):
        def one(source, carry):
            d_forward(half, 1 - core, source).wait_recv()
            return carry

        return one

    square_of = acc_gu.at[2]

    def lift(half, parity):
        for k in range(4):
            at = pl.multiple_of((2 * relative(4 * half + k) + parity) * COLS, COLS)
            block = dbuf[pl.ds(parity, 1), half, :, k].reshape(NEP, 16, 128)
            low, high = halves_beside(block)
            square_of[:, :128] += low * low + high * high
            both = jnp.concatenate([low, high], axis=1) * v_ffn_gain[:, pl.ds(at, COLS)]
            lifted[:, k * COLS : (k + 1) * COLS] = both.astype(BF16)
        at = pl.multiple_of((parity * NZ + 4 * half) * COLS, 4 * COLS)
        for j in range(2):
            acc_gu[j] += jnp.dot(
                lifted[...], v_gu[j, pl.ds(at, 4 * COLS), :], preferred_element_type=F32
            )

    mark("d_wait0")
    d_arrive(0)
    lax.fori_loop(0, NTP, lift_loaded, 0)
    mark("lift_own0")
    lift(0, core)
    mark("d_wait1")
    d_arrive(1)
    lax.fori_loop(0, NEP, d_other_wait(0), 0)
    mark("lift_other0")
    lift(0, 1 - core)
    mark("lift_own1")
    lift(1, core)
    mark("lift_wait")
    lax.fori_loop(0, NEP, d_other_wait(1), 0)
    mark("lift_other1")
    lift(1, 1 - core)
    mark("act")
    inner = lax.rsqrt(
        jnp.sum(square_of[:, :128], axis=-1, keepdims=True) * (1.0 / D) + EPS
    )
    own_expert = lax.broadcasted_iota(jnp.int32, (SLOTS, COLS), 0) % 8 < 4
    chosen = jnp.where(own_expert, acc_gu[0], acc_gu[1]) * inner
    activated = jax.nn.silu(chosen[:, :128]) * chosen[:, 128:]
    ebuf[pl.ds(tp, 1)] = activated.astype(BF16).reshape(1, SLOTS, 128)
    copies[14].wait()

    def lower(row, first_step):
        @pl.when(first_step)
        def _():
            acc_down[...] = jnp.zeros_like(acc_down)

        pair = ebuf[pl.ds(2 * row, 2)]
        both = jnp.concatenate([pair[0], pair[1]], axis=1)
        at = pl.multiple_of(row * COLS, COLS)
        for j in range(2):
            acc_down[j] += jnp.dot(both, v_down[j, pl.ds(at, COLS), :], preferred_element_type=F32)

    mark("e_gather")
    finish_e = gather(ebuf, e_send, e_fwd, e_recv, lower)
    mark("result")
    result = jnp.where(own_expert, acc_down[0], acc_down[1])

    fsend[...] = halves_below(result).astype(BF16)

    def f_copy(peer, source):
        return copy_to(
            fsend.at[peer], frecv.at[source], f_send.at[peer], f_recv.at[source], peer, tp
        )

    for peer in plane[:0:-1]:
        f_copy(peer, ep).start()
    frecv[pl.ds(ep, 1)] = fsend[pl.ds(ep, 1)]

    mark("sent")
    def sent_ring(i, carry):
        a1_copy(i, z).wait_send()
        g_copy(i, z).wait_send()
        return carry

    lax.fori_loop(0, NZ - 1, sent_ring, 0)

    for row in range(4):
        for cc in range(2):

            @pl.when((row != down) | (cc != core))
            def _():
                a2_copy(row, cc).wait_send()

    for copy in w_sends:
        copy.wait_send()

    def sent_b(i, carry):
        b_copy(down, (down + near(i)) % 4).wait_send()
        return carry

    lax.fori_loop(1, 4, sent_b, 0)
    ss_copy.wait_send()
    for half in range(2):
        d_forward(half, core, ep).wait_send()

    def sent_plane(i, carry):
        peer = (ep + i) % NEP
        for half in range(2):
            d_copy(half, peer, ep).wait_send()
            d_forward(half, core, peer).wait_send()
        return carry

    lax.fori_loop(1, NEP, sent_plane, 0)
    finish_c()
    finish_e()

    def f_wait(i, carry):
        peer = (ep + i) % NEP
        f_copy(peer, peer).wait_recv()
        return carry

    mark("f_wait")
    lax.fori_loop(1, NEP, f_wait, 0)
    mark("combine")
    back = jnp.concatenate(halves_beside(frecv[...]), axis=1)
    weighted = jnp.dot(
        combine, back, preferred_element_type=F32, precision=lax.Precision.HIGHEST
    )
    updated[...] = (after.astype(F32) + weighted).astype(BF16)

    def f_sent(i, carry):
        f_copy((ep + i) % NEP, ep).wait_send()
        return carry

    lax.fori_loop(1, NEP, f_sent, 0)
    mark("")


def state_body(before, state, updated, next_state, sem):
    copies = [
        pltpu.make_async_copy(before, updated, sem.at[0]),
        pltpu.make_async_copy(state, next_state, sem.at[1]),
    ]
    for copy in copies:
        copy.start()
    for copy in copies:
        copy.wait()


def per_device(
    hidden,
    positions,
    ret_state,
    query_weight,
    key_weight,
    value_weight,
    gate_weight,
    head_gain,
    out_weight,
    mix_gain,
    ffn_gain,
    expert_gate,
    expert_up,
    expert_down,
    route_ids,
    route_weight,
):
    table = jnp.asarray(constants())
    dma = pltpu.SemaphoreType.DMA
    vmem = pltpu.VMEM
    anywhere = pl.BlockSpec(memory_space=pltpu.HBM)
    updated, parts = pl.pallas_call(
        body,
        out_shape=(
            pltpu.VMEM((ROWS, COLS), BF16),
            pltpu.VMEM(ret_state.shape, F32),
        ),
        in_specs=[anywhere] * 17,
        out_specs=(pl.BlockSpec(memory_space=pltpu.VMEM),) * 2,
        scratch_shapes=[
            vmem((ROWS, COLS), BF16),
            vmem((1, ROWS), jnp.int32),
            vmem((4, COLS, 512), BF16),
            vmem((1, HEAD), F32),
            vmem((RD, COLS), BF16),
            vmem((1, D), F32),
            vmem((1, D), F32),
            vmem((2, D, COLS), BF16),
            vmem((2, RD, COLS), BF16),
            vmem((2, ROWS), jnp.int32),
            vmem((2, ROWS), F32),
            vmem((24, 128), F32),
            vmem((NZ, ROWS, COLS), BF16),
            vmem((4, 2, 2, ROWS, COLS), BF16),
            vmem((4 * ROWS, 512), F32),
            vmem((4, ROWS, 512), BF16),
            vmem((4, ROWS, 512), BF16),
            vmem((ROWS, 128), F32),
            vmem((ROWS, 128), F32),
            vmem((4, ROWS, HEAD), F32),
            vmem((NTP, ROWS, HEAD), BF16),
            vmem((NZ, ROWS, COLS), BF16),
            vmem((2, NEP, 4, 16, 128), BF16),
            vmem((2, 2, NEP, 4, 16, 128), BF16),
            vmem((SLOTS, 4 * COLS), BF16),
            vmem((3, SLOTS, COLS), F32),
            vmem((NTP, SLOTS, 128), BF16),
            vmem((2, SLOTS, COLS), F32),
            vmem((NEP, 16, 128), BF16),
            vmem((NEP, 16, 128), BF16),
            dma((15,)),
            dma((NTP, 2)),
            dma((2, 3)),
            dma((4, 2)),
            dma((NZ,)),
            dma((NZ,)),
            dma((4, 2)),
            dma((4, 2)),
            dma((2,)),
            dma((4,)),
            dma((4,)),
            dma((NZ,)),
            dma((NZ,)),
            dma((NTP,)),
            dma((NZ,)),
            dma((NZ,)),
            dma((2, NEP)),
            dma((2, NEP)),
            dma((2, NEP)),
            dma((2, NEP)),
            dma((NZ,)),
            dma((NZ,)),
            dma((NTP,)),
            dma((NEP,)),
            dma((NEP,)),
        ],
        compiler_params=pltpu.CompilerParams(
            collective_id=0, has_side_effects=True, vmem_limit_bytes=LIMIT
        ),
    )(
        hidden,
        positions.reshape(1, ROWS),
        ret_state,
        query_weight,
        key_weight,
        value_weight,
        gate_weight,
        head_gain.reshape(1, HEAD),
        out_weight,
        mix_gain.reshape(1, D),
        ffn_gain.reshape(1, D),
        expert_gate,
        expert_up,
        expert_down,
        route_ids.T,
        route_weight.T,
        table,
    )
    return pl.pallas_call(
        state_body,
        out_shape=(
            jax.ShapeDtypeStruct((ROWS, COLS), BF16),
            jax.ShapeDtypeStruct(ret_state.shape, F32),
        ),
        in_specs=[pl.BlockSpec(memory_space=pl.ANY)] * 2,
        out_specs=(anywhere,) * 2,
        scratch_shapes=[dma((2,))],
        compiler_params=pltpu.CompilerParams(vmem_limit_bytes=1024 * 1024),
    )(updated, parts)


def solution(mesh):
    return jax.shard_map(
        per_device,
        mesh=mesh,
        in_specs=(
            P("ep", "tp"),
            P("ep"),
            P("ep", "tp", None, None),
            P("ep", "tp"),
            P("ep", "tp"),
            P("ep", "tp"),
            P("ep", "tp"),
            P("tp"),
            P(None, "tp"),
            P(),
            P(),
            P("ep", None, "tp"),
            P("ep", None, "tp"),
            P("ep", None, "tp"),
            P("ep", None),
            P("ep", None),
        ),
        out_specs=(P("ep", "tp"), P("ep", "tp", None, None)),
        check_vma=False,
    )
```

```python
import functools

import jax
import jax.numpy as jnp
import numpy as np
from jax import lax
from jax.experimental import pallas as pl
from jax.experimental.pallas import tpu as pltpu
from jax.sharding import PartitionSpec as P

MESH = pl.DeviceIdType.MESH
F32 = jnp.float32
BF16 = jnp.bfloat16
D = 4096
RD = 2048
HEADS = 16
HEAD = 128
ROWS = 40
COLS = 256
NEP = 16
NTP = 16
NZ = 8
SLOTS = 128
LIMIT = 67043328 - 40 * 128 * 128 * 4 - 2 * 16384 * 2
GROUPS_OF_ROWS = ROWS // 8
EPS = 1e-06


def constants():
    table = np.zeros((24, 128), np.float64)
    heads = np.arange(HEADS, dtype=np.float64)
    table[:HEADS] = (1.0 - 2.0 ** (-5.0 - 5.0 * heads / (HEADS - 1)))[:, None]
    inverse = 10000.0 ** (-np.arange(0, HEAD, 2, dtype=np.float64) / HEAD)
    table[HEADS] = np.concatenate([inverse, inverse])
    return table.astype(np.float32)


TRACE = False
_open = []


def mark(name):
    if not TRACE:
        return
    while _open:
        _open.pop().__exit__(None, None, None)
    if name:
        _open.append(jax.named_scope(name))
        _open[-1].__enter__()


def ring_offset(i):
    half = i // 2 + 1
    return half + ((i + 1) % 2) * (NZ - 2 * half)


def body(
    hidden,
    positions,
    ret_state,
    query_weight,
    key_weight,
    value_weight,
    gate_weight,
    head_gain,
    out_weight,
    mix_gain,
    ffn_gain,
    expert_gate,
    expert_up,
    expert_down,
    route_ids,
    route_weight,
    table,
    updated,
    v_state,
    v_hidden,
    v_pos,
    v_qkvg,
    v_head_gain,
    v_out,
    v_mix_gain,
    v_ffn_gain,
    v_gu,
    v_down,
    v_ids,
    v_weight,
    v_table,
    agbuf,
    xbuf,
    bacc,
    bsend,
    brecv,
    ssout,
    ssin,
    readbuf,
    spread,
    cbuf,
    afters,
    psend,
    dbuf,
    lifted,
    acc_gu,
    ebuf,
    acc_down,
    fsend,
    frecv,
    local_sem,
    gu_sem,
    w_send,
    w_recv,
    a1_send,
    a1_recv,
    a2_send,
    a2_recv,
    ss_sem,
    b_send,
    b_recv,
    c_send,
    c_fwd,
    c_recv,
    g_send,
    g_recv,
    d_send,
    d_fwd,
    d_recv,
    d_other,
    e_send,
    e_fwd,
    e_recv,
    f_send,
    f_recv,
):
    ep = lax.axis_index("ep")
    tp = lax.axis_index("tp")
    z = tp // 2
    core = tp % 2
    other = 2 * z + 1 - core
    down = ep // 4
    across = ep % 4

    mark("load")
    loads = [
        (hidden, v_hidden),
        (positions, v_pos),
        (table, v_table),
        (route_ids, v_ids),
        (route_weight, v_weight),
        (head_gain, v_head_gain),
        (mix_gain, v_mix_gain),
        (ffn_gain, v_ffn_gain),
        (query_weight, v_qkvg.at[across, :, pl.ds(0, 128)]),
        (key_weight, v_qkvg.at[across, :, pl.ds(128, 128)]),
        (value_weight, v_qkvg.at[across, :, pl.ds(256, 128)]),
        (gate_weight, v_qkvg.at[across, :, pl.ds(384, 128)]),
        (ret_state, v_state),
        (out_weight, v_out),
        (expert_down, v_down),
    ]
    copies = [pltpu.make_async_copy(src, dst, local_sem.at[i]) for i, (src, dst) in enumerate(loads)]
    for copy in copies[:12]:
        copy.start()

    def relative(i):
        return (z + (i + 1) // 2 * (1 - i % 2 * 2) + NZ) % NZ

    def lift_load(i, up):
        parity, place = i // NZ, i % NZ
        source = pl.multiple_of((2 * relative(place) + parity) * COLS, COLS)
        return pltpu.make_async_copy(
            (expert_up if up else expert_gate).at[:, pl.ds(source, COLS)],
            v_gu.at[:, pl.ds(pl.multiple_of(i * COLS, COLS), COLS), pl.ds(128 * up, 128)],
            gu_sem.at[i, up],
        )

    def lift_loads(i, carry):
        lift_load(i, 0).start()
        lift_load(i, 1).start()
        return carry

    def lift_loaded(i, carry):
        lift_load(i, 0).wait()
        lift_load(i, 1).wait()
        return carry

    barrier = pltpu.get_barrier_semaphore()

    def greet_plane(i, carry):
        peer = (ep + i) % NEP
        pl.semaphore_signal(barrier, inc=1, device_id=(peer, tp), device_id_type=MESH)
        pl.semaphore_signal(barrier, inc=1, device_id=(peer, other), device_id_type=MESH)
        return carry

    def greet_ring(i, carry):
        peer = 2 * ((z + i) % NZ) + core
        pl.semaphore_signal(barrier, inc=1, device_id=(ep, peer), device_id_type=MESH)
        return carry

    lax.fori_loop(1, NEP, greet_plane, 0)
    lax.fori_loop(1, NZ, greet_ring, 0)
    pl.semaphore_signal(barrier, inc=1, device_id=(ep, other), device_id_type=MESH)
    for copy in copies[12:]:
        copy.start()
    lax.fori_loop(0, NTP, lift_loads, 0)
    for copy in copies[:8]:
        copy.wait()
    agbuf[pl.ds(z, 1)] = v_hidden[...].reshape(1, ROWS, COLS)

    mark("prep")
    token = lax.broadcasted_iota(jnp.int32, (ROWS, ROWS), 0)
    other_token = lax.broadcasted_iota(jnp.int32, (ROWS, ROWS), 1)

    def column(row):
        return jnp.sum(jnp.where(token == other_token, row.astype(F32), 0.0), axis=1, keepdims=True)

    inverse = v_table[HEADS : HEADS + 1, :]
    angle = column(v_pos[...]) * inverse
    cosine = jnp.cos(angle)
    sine = jnp.sin(angle)
    lane = lax.broadcasted_iota(jnp.int32, (ROWS, 128), 1)
    sine = jnp.where(lane < HEAD // 2, -sine, sine)

    slot_expert = lane // 4
    slot_expert = slot_expert.astype(F32)
    first = column(v_ids[0:1, :]) == slot_expert
    second = column(v_ids[1:2, :]) == slot_expert
    named = jnp.where(first | second, 1.0, 0.0).astype(F32)
    earlier = jnp.where(token > other_token, 1.0, 0.0).astype(BF16)
    ranks = jnp.dot(earlier, named.astype(BF16), preferred_element_type=F32)
    placed = jnp.where(ranks == (lane % 4).astype(F32), named, 0.0)
    combine = placed * jnp.where(first, column(v_weight[0:1, :]), column(v_weight[1:2, :]))

    mark("barrier")
    pl.semaphore_wait(barrier, 2 * (NEP - 1) + (NZ - 1) + 1)

    def copy_to(src, dst, send_sem, recv_sem, to_ep, to_tp):
        return pltpu.make_async_remote_copy(
            src_ref=src,
            dst_ref=dst,
            send_sem=send_sem,
            recv_sem=recv_sem,
            device_id=(to_ep, to_tp),
            device_id_type=MESH,
        )

    right = 4 * down + (across + 1) % 4
    left = 4 * down + (across + 3) % 4

    def w_copy(block, half, way, i):
        part = v_qkvg.at[block, pl.ds(half * 128, 128)]
        return copy_to(
            part, part, w_send.at[way, i], w_recv.at[block, half], right if way == 0 else left, tp
        )

    for copy in copies[8:12]:
        copy.wait()
    w_sends = [
        w_copy(across, 0, 0, 0),
        w_copy(across, 1, 1, 0),
        w_copy(across, 1, 0, 1),
        w_copy(across, 0, 1, 1),
        w_copy(left % 4, 0, 0, 2),
        w_copy(right % 4, 1, 1, 2),
    ]

    def a1_copy(i, slot):
        peer = 2 * ((z + ring_offset(i)) % NZ) + core
        return copy_to(v_hidden, agbuf.at[slot], a1_send.at[i], a1_recv.at[slot], ep, peer)

    def a1_start(i, carry):
        a1_copy(NZ - 2 - i, z).start()
        return carry

    lax.fori_loop(0, NZ - 1, a1_start, 0)
    for copy in w_sends[:4]:
        copy.start()

    def near(i):
        return i + (i // 2) * (5 - 2 * i)

    def a2_copy(row, cc):
        return copy_to(
            agbuf.at[pl.ds(2 * row, 2)],
            xbuf.at[down, core],
            a2_send.at[row, cc],
            a2_recv.at[down, core],
            4 * row + across,
            2 * z + cc,
        )

    def a2_start(i, carry):
        row = (z // 2 + near(i)) % 4
        for k in range(2):
            slot = 2 * row + k

            @pl.when(slot != z)
            def _():
                a1_copy(0, slot).wait_recv()

        for cc in range(2):
            mine = (row == down) & (cc == core)

            @pl.when(jnp.logical_not(mine))
            def _():
                a2_copy(row, cc).start()

            @pl.when(mine)
            def _():
                xbuf[pl.ds(row, 1), pl.ds(core, 1)] = agbuf[pl.ds(2 * row, 2)].reshape(
                    1, 1, 2, ROWS, COLS
                )

        return carry

    mark("a1_wait_a2_issue")
    lax.fori_loop(0, 4, a2_start, 0)
    mark("w_forward")
    w_copy(left % 4, 0, 0, 0).wait_recv()
    w_sends[4].start()
    w_copy(right % 4, 1, 1, 0).wait_recv()
    w_sends[5].start()

    mark("ss")
    def square(i, total):
        part = agbuf[pl.ds(i, 1)].reshape(ROWS, COLS).astype(F32)
        part = part * part
        return total + part[:, :128] + part[:, 128:]

    ssout[...] = lax.fori_loop(0, NZ, square, jnp.zeros((ROWS, 128), F32))
    ss_copy = copy_to(ssout, ssin, ss_sem.at[0], ss_sem.at[1], ep, other)
    ss_copy.start()

    steps = (0, 1, 3, 2)
    plane = [
        4 * lax.rem(down + row, 4) + lax.rem(across + column_step, 4)
        for row in steps
        for column_step in steps
    ]

    def b_copy(slot, row):
        return copy_to(
            bsend.at[row], brecv.at[slot], b_send.at[row], b_recv.at[slot], 4 * row + across, tp
        )

    mark("a2_wait")
    for row in range(4):
        for parity in range(2):

            @pl.when((row != down) | (parity != core))
            def _():
                block = xbuf.at[row, parity]
                copy_to(block, block, a2_send.at[0, 0], a2_recv.at[row, parity], ep, other).wait_recv()

    def partial(block):
        at = pl.multiple_of((4 * down + block) * COLS, COLS)
        gain = v_mix_gain[:, pl.ds(at, COLS)].reshape(1, 1, COLS)
        rows = xbuf[:, pl.ds(block % 2, 1), pl.ds(block // 2, 1)].reshape(4, ROWS, COLS)
        rows = (rows.astype(F32) * gain).reshape(4 * ROWS, COLS).astype(BF16)
        return jnp.dot(
            rows, v_qkvg[pl.ds(block, 1)].reshape(COLS, 512), preferred_element_type=F32
        )

    mark("b_rows")
    bacc[...] = partial(across)
    w_copy(left % 4, 1, 0, 0).wait_recv()
    bacc[...] += partial(left % 4)
    w_copy(right % 4, 0, 1, 0).wait_recv()
    bacc[...] += partial(right % 4)
    opposite = (across + 2) % 4
    mark("w_wait")
    w_copy(opposite, 0, 0, 0).wait_recv()
    w_copy(opposite, 1, 1, 0).wait_recv()
    mark("b_last")
    bsend[...] = (bacc[...] + partial(opposite)).reshape(4, ROWS, 512).astype(BF16)

    def b_start(i, carry):
        b_copy(down, (down + near(3 - i)) % 4).start()
        return carry

    lax.fori_loop(0, 3, b_start, 0)
    brecv[pl.ds(down, 1)] = bsend[pl.ds(down, 1)]

    mark("ss_wait")
    ss_copy.wait_recv()
    square_sum = jnp.sum(ssout[...] + ssin[...], axis=-1, keepdims=True)
    factor = lax.rsqrt(square_sum * (1.0 / D) + EPS)

    mark("b_sum")

    def b_wait(i, carry):
        row = (down + near(i)) % 4
        b_copy(row, row).wait_recv()
        return carry

    lax.fori_loop(1, 4, b_wait, 0)
    part = brecv[...].astype(F32)
    joined = (part[0] + part[1]) + (part[2] + part[3])
    joined = (joined * factor).astype(BF16).astype(F32)

    mark("rot")
    def rotate(values):
        return values * cosine + pltpu.roll(values, HEAD // 2, 1) * sine

    rotated_query = rotate(joined[:, :128])
    rotated_key = rotate(joined[:, 128:256]) * HEAD ** (-0.5)
    value = joined[:, 256:384]
    gate_rows = joined[:, 384:]
    decay = v_table[pl.ds(tp, 1), :]
    readbuf[0] = rotated_query
    readbuf[1] = rotated_key
    readbuf[2] = value
    mark("retain")
    copies[12].wait()

    own_block = (
        lax.rem(lax.broadcasted_iota(jnp.int32, (32, 8 * HEAD), 0), 8)
        == lax.broadcasted_iota(jnp.int32, (32, 8 * HEAD), 1) // HEAD
    )
    spread[...] = jnp.where(own_block, 1.0, 0.0).astype(BF16)

    def terms(rows):
        high = rows.astype(BF16).astype(F32)
        middle = (rows - high).astype(BF16).astype(F32)
        low = rows - high - middle
        return jnp.concatenate([high, middle, low, jnp.zeros_like(rows)], axis=0).astype(BF16)

    def over_rows(stack, columns):
        return lax.dot_general(
            stack, columns, (((0,), (0,)), ((), ())), preferred_element_type=F32
        )

    def retain(group, carry):
        at = pl.ds(pl.multiple_of(8 * group, 8), 8)
        values = jnp.concatenate([readbuf[2, at, :]] * 4, axis=0)
        values = jnp.where(own_block, jnp.concatenate([values] * 8, axis=1), 0.0).astype(BF16)
        outer = over_rows(terms(readbuf[1, at, :]), values)
        query = over_rows(terms(readbuf[0, at, :]), spread[...])
        reads = []
        for k in range(8):
            block = slice(k * HEAD, (k + 1) * HEAD)
            state = decay * v_state[8 * group + k, 0] + outer[:, block]
            v_state[8 * group + k, 0] = state
            reads.append(jnp.sum(query[:, block] * state, axis=0, keepdims=True))
        readbuf[3, at, :] = jnp.concatenate(reads, axis=0)
        return carry

    lax.fori_loop(0, ROWS // 8, retain, 0)
    mark("groupnorm")
    read = readbuf[3]
    centered = read - jnp.mean(read, axis=-1, keepdims=True)
    normal = centered * lax.rsqrt(jnp.mean(centered * centered, axis=-1, keepdims=True) + EPS)
    mixed = normal * v_head_gain[...] * jax.nn.silu(gate_rows)
    cbuf[pl.ds(tp, 1)] = mixed.astype(BF16).reshape(1, ROWS, HEAD)

    def gather(buf, send_sem, fwd_sem, recv_sem, consume, both=False, lag=0):
        def direct(i, slot):
            peer = 2 * ((z + ring_offset(i)) % NZ) + core
            return copy_to(buf.at[slot], buf.at[slot], send_sem.at[i], recv_sem.at[slot], ep, peer)

        def forward(row, slot):
            return copy_to(
                buf.at[slot], buf.at[slot], fwd_sem.at[row], recv_sem.at[slot], ep, other
            )

        def cross(i, slot):
            peer = 2 * lax.rem(z + ring_offset(i), NZ) + 1 - core
            return copy_to(
                buf.at[slot], buf.at[slot], fwd_sem.at[i], recv_sem.at[slot], ep, peer
            )

        def begin(i, carry):
            direct(i, tp).start()
            if both:
                cross(i, tp).start()
            return carry

        lax.fori_loop(0, NZ - 1, begin, 0)
        forward(NZ - 1 if both else z, tp).start()

        def step(i, carry):
            @pl.when(i < NZ - 1)
            def _():
                row = (z + ring_offset(i)) % NZ
                direct(0, 2 * row + core).wait_recv()
                if not both:
                    forward(row, 2 * row + core).start()

            @pl.when(i >= lag)
            def _():
                place = i - lag
                before = relative(place)
                forward(before, 2 * before + 1 - core).wait_recv()
                consume(before, place == 0)

            return carry

        lax.fori_loop(0, NZ + lag, step, 0)

        def finish():
            def one(i, carry):
                direct(i, tp).wait_send()
                forward(i if both else (z + ring_offset(i)) % NZ, tp).wait_send()
                return carry

            lax.fori_loop(0, NZ - 1, one, 0)
            forward(NZ - 1 if both else z, tp).wait_send()

        return finish

    copies[13].wait()
    projected = readbuf.at[pl.ds(0, 2)]

    def project(row, first_step):
        pair = cbuf[pl.ds(2 * row, 2)].astype(F32)
        block = jnp.concatenate([pair[0], pair[1]], axis=1).astype(BF16)
        part = jnp.dot(
            block,
            v_out[pl.ds(pl.multiple_of(row * COLS, COLS), COLS), :],
            preferred_element_type=F32,
        )

        @pl.when(first_step)
        def _():
            projected[0] = part[:, :128]
            projected[1] = part[:, 128:]

        @pl.when(jnp.logical_not(first_step))
        def _():
            projected[0] += part[:, :128]
            projected[1] += part[:, 128:]

    mark("c_gather")
    finish_c = gather(cbuf, c_send, c_fwd, c_recv, project, both=True)
    mark("after_pack")
    own = v_hidden[...].astype(F32)
    after = (own + jnp.concatenate([projected[0], projected[1]], axis=1)).astype(BF16)
    afters[pl.ds(z, 1)] = after.reshape(1, ROWS, COLS)

    def g_copy(i, slot):
        peer = 2 * ((z + ring_offset(i)) % NZ) + core
        return copy_to(afters.at[z], afters.at[slot], g_send.at[i], g_recv.at[slot], ep, peer)

    def g_start(i, carry):
        g_copy(i, z).start()
        return carry

    lax.fori_loop(0, NZ - 1, g_start, 0)

    def halves_below(array):
        parts = [array[:, :128].reshape(NEP, 8, 128), array[:, 128:].reshape(NEP, 8, 128)]
        return jnp.concatenate(parts, axis=1)

    def halves_beside(array):
        array = array.astype(F32)
        return array[:, :8].reshape(SLOTS, 128), array[:, 8:].reshape(SLOTS, 128)

    placing = placed.astype(BF16)

    def pack(half, k):
        packed = lax.dot_general(
            placing,
            afters[pl.ds(relative(4 * half + k), 1)].reshape(ROWS, COLS),
            (((0,), (0,)), ((), ())),
            preferred_element_type=F32,
        )
        packed = halves_below(packed).astype(BF16)
        psend[half, :, pl.ds(k, 1)] = packed.reshape(NEP, 1, 16, 128)

    def d_copy(half, peer, source):
        return copy_to(
            psend.at[half, peer],
            dbuf.at[core, half, source],
            d_send.at[half, peer],
            d_recv.at[half, source],
            peer,
            tp,
        )

    def d_forward(half, parity, source):
        block = dbuf.at[parity, half, source]
        return copy_to(block, block, d_fwd.at[half, source], d_other.at[half, source], ep, other)

    def pack_next(half):
        def one(k, carry):
            g_copy(4 * half + k - 1, relative(4 * half + k)).wait_recv()
            pack(half, k)
            return carry

        return one

    pack(0, 0)
    acc_gu[...] = jnp.zeros_like(acc_gu)
    for half in range(2):
        mark(f"after_gather{half}")
        lax.fori_loop(1 - half, 4, pack_next(half), 0)
        mark(f"d_issue{half}")
        for peer in plane[:0:-1]:
            d_copy(half, peer, ep).start()
        dbuf[pl.ds(core, 1), half, pl.ds(ep, 1)] = psend[half, pl.ds(ep, 1)].reshape(
            1, 1, 4, 16, 128
        )
        d_forward(half, core, ep).start()

    def d_arrive(half):
        for peer in plane[1:]:
            d_copy(half, peer, peer).wait_recv()
            d_forward(half, core, peer).start()

    def d_other_wait(half):
        def one(source, carry):
            d_forward(half, 1 - core, source).wait_recv()
            return carry

        return one

    square_of = acc_gu.at[2]

    def lift(half, parity):
        for k in range(4):
            at = pl.multiple_of((2 * relative(4 * half + k) + parity) * COLS, COLS)
            block = dbuf[pl.ds(parity, 1), half, :, k].reshape(NEP, 16, 128)
            low, high = halves_beside(block)
            square_of[:, :128] += low * low + high * high
            both = jnp.concatenate([low, high], axis=1) * v_ffn_gain[:, pl.ds(at, COLS)]
            lifted[:, k * COLS : (k + 1) * COLS] = both.astype(BF16)
        at = pl.multiple_of((parity * NZ + 4 * half) * COLS, 4 * COLS)
        for j in range(2):
            acc_gu[j] += jnp.dot(
                lifted[...], v_gu[j, pl.ds(at, 4 * COLS), :], preferred_element_type=F32
            )

    mark("d_wait0")
    d_arrive(0)
    lax.fori_loop(0, NTP, lift_loaded, 0)
    mark("lift_own0")
    lift(0, core)
    mark("d_wait1")
    d_arrive(1)
    lax.fori_loop(0, NEP, d_other_wait(0), 0)
    mark("lift_other0")
    lift(0, 1 - core)
    mark("lift_own1")
    lift(1, core)
    mark("lift_wait")
    lax.fori_loop(0, NEP, d_other_wait(1), 0)
    mark("lift_other1")
    lift(1, 1 - core)
    mark("act")
    inner = lax.rsqrt(
        jnp.sum(square_of[:, :128], axis=-1, keepdims=True) * (1.0 / D) + EPS
    )
    own_expert = lax.broadcasted_iota(jnp.int32, (SLOTS, COLS), 0) % 8 < 4
    chosen = jnp.where(own_expert, acc_gu[0], acc_gu[1]) * inner
    activated = jax.nn.silu(chosen[:, :128]) * chosen[:, 128:]
    ebuf[pl.ds(tp, 1)] = activated.astype(BF16).reshape(1, SLOTS, 128)
    copies[14].wait()

    def lower(row, first_step):
        @pl.when(first_step)
        def _():
            acc_down[...] = jnp.zeros_like(acc_down)

        pair = ebuf[pl.ds(2 * row, 2)]
        both = jnp.concatenate([pair[0], pair[1]], axis=1)
        at = pl.multiple_of(row * COLS, COLS)
        for j in range(2):
            acc_down[j] += jnp.dot(both, v_down[j, pl.ds(at, COLS), :], preferred_element_type=F32)

    mark("e_gather")
    finish_e = gather(ebuf, e_send, e_fwd, e_recv, lower, lag=1)
    mark("result")
    result = jnp.where(own_expert, acc_down[0], acc_down[1])

    fsend[...] = halves_below(result).astype(BF16)

    def f_copy(peer, source):
        return copy_to(
            fsend.at[peer], frecv.at[source], f_send.at[peer], f_recv.at[source], peer, tp
        )

    for peer in plane[:0:-1]:
        f_copy(peer, ep).start()
    frecv[pl.ds(ep, 1)] = fsend[pl.ds(ep, 1)]

    mark("sent")
    def sent_ring(i, carry):
        a1_copy(i, z).wait_send()
        g_copy(i, z).wait_send()
        return carry

    lax.fori_loop(0, NZ - 1, sent_ring, 0)

    for row in range(4):
        for cc in range(2):

            @pl.when((row != down) | (cc != core))
            def _():
                a2_copy(row, cc).wait_send()

    for copy in w_sends:
        copy.wait_send()

    def sent_b(i, carry):
        b_copy(down, (down + near(i)) % 4).wait_send()
        return carry

    lax.fori_loop(1, 4, sent_b, 0)
    ss_copy.wait_send()
    for half in range(2):
        d_forward(half, core, ep).wait_send()

    def sent_plane(i, carry):
        peer = (ep + i) % NEP
        for half in range(2):
            d_copy(half, peer, ep).wait_send()
            d_forward(half, core, peer).wait_send()
        return carry

    lax.fori_loop(1, NEP, sent_plane, 0)
    finish_c()
    finish_e()

    def f_wait(i, carry):
        peer = (ep + i) % NEP
        f_copy(peer, peer).wait_recv()
        return carry

    mark("f_wait")
    lax.fori_loop(1, NEP, f_wait, 0)
    mark("combine")
    back = jnp.concatenate(halves_beside(frecv[...]), axis=1)
    weighted = jnp.dot(
        combine, back, preferred_element_type=F32, precision=lax.Precision.HIGHEST
    )
    updated[...] = (after.astype(F32) + weighted).astype(BF16)

    def f_sent(i, carry):
        f_copy((ep + i) % NEP, ep).wait_send()
        return carry

    lax.fori_loop(1, NEP, f_sent, 0)
    mark("")


def state_body(before, state, updated, next_state, sem):
    copies = [
        pltpu.make_async_copy(before, updated, sem.at[0]),
        pltpu.make_async_copy(state, next_state, sem.at[1]),
    ]
    for copy in copies:
        copy.start()
    for copy in copies:
        copy.wait()


def per_device(
    hidden,
    positions,
    ret_state,
    query_weight,
    key_weight,
    value_weight,
    gate_weight,
    head_gain,
    out_weight,
    mix_gain,
    ffn_gain,
    expert_gate,
    expert_up,
    expert_down,
    route_ids,
    route_weight,
):
    table = jnp.asarray(constants())
    dma = pltpu.SemaphoreType.DMA
    vmem = pltpu.VMEM
    anywhere = pl.BlockSpec(memory_space=pltpu.HBM)
    updated, parts = pl.pallas_call(
        body,
        out_shape=(
            pltpu.VMEM((ROWS, COLS), BF16),
            pltpu.VMEM(ret_state.shape, F32),
        ),
        in_specs=[anywhere] * 17,
        out_specs=(pl.BlockSpec(memory_space=pltpu.VMEM),) * 2,
        scratch_shapes=[
            vmem((ROWS, COLS), BF16),
            vmem((1, ROWS), jnp.int32),
            vmem((4, COLS, 512), BF16),
            vmem((1, HEAD), F32),
            vmem((RD, COLS), BF16),
            vmem((1, D), F32),
            vmem((1, D), F32),
            vmem((2, D, COLS), BF16),
            vmem((2, RD, COLS), BF16),
            vmem((2, ROWS), jnp.int32),
            vmem((2, ROWS), F32),
            vmem((24, 128), F32),
            vmem((NZ, ROWS, COLS), BF16),
            vmem((4, 2, 2, ROWS, COLS), BF16),
            vmem((4 * ROWS, 512), F32),
            vmem((4, ROWS, 512), BF16),
            vmem((4, ROWS, 512), BF16),
            vmem((ROWS, 128), F32),
            vmem((ROWS, 128), F32),
            vmem((4, ROWS, HEAD), F32),
            vmem((32, 8 * HEAD), BF16),
            vmem((NTP, ROWS, HEAD), BF16),
            vmem((NZ, ROWS, COLS), BF16),
            vmem((2, NEP, 4, 16, 128), BF16),
            vmem((2, 2, NEP, 4, 16, 128), BF16),
            vmem((SLOTS, 4 * COLS), BF16),
            vmem((3, SLOTS, COLS), F32),
            vmem((NTP, SLOTS, 128), BF16),
            vmem((2, SLOTS, COLS), F32),
            vmem((NEP, 16, 128), BF16),
            vmem((NEP, 16, 128), BF16),
            dma((15,)),
            dma((NTP, 2)),
            dma((2, 3)),
            dma((4, 2)),
            dma((NZ,)),
            dma((NZ,)),
            dma((4, 2)),
            dma((4, 2)),
            dma((2,)),
            dma((4,)),
            dma((4,)),
            dma((NZ,)),
            dma((NZ,)),
            dma((NTP,)),
            dma((NZ,)),
            dma((NZ,)),
            dma((2, NEP)),
            dma((2, NEP)),
            dma((2, NEP)),
            dma((2, NEP)),
            dma((NZ,)),
            dma((NZ,)),
            dma((NTP,)),
            dma((NEP,)),
            dma((NEP,)),
        ],
        compiler_params=pltpu.CompilerParams(
            collective_id=0, has_side_effects=True, vmem_limit_bytes=LIMIT
        ),
    )(
        hidden,
        positions.reshape(1, ROWS),
        ret_state,
        query_weight,
        key_weight,
        value_weight,
        gate_weight,
        head_gain.reshape(1, HEAD),
        out_weight,
        mix_gain.reshape(1, D),
        ffn_gain.reshape(1, D),
        expert_gate,
        expert_up,
        expert_down,
        route_ids.T,
        route_weight.T,
        table,
    )
    return pl.pallas_call(
        state_body,
        out_shape=(
            jax.ShapeDtypeStruct((ROWS, COLS), BF16),
            jax.ShapeDtypeStruct(ret_state.shape, F32),
        ),
        in_specs=[pl.BlockSpec(memory_space=pl.ANY)] * 2,
        out_specs=(anywhere,) * 2,
        scratch_shapes=[dma((2,))],
        compiler_params=pltpu.CompilerParams(vmem_limit_bytes=1024 * 1024),
    )(updated, parts)


def solution(mesh):
    return jax.shard_map(
        per_device,
        mesh=mesh,
        in_specs=(
            P("ep", "tp"),
            P("ep"),
            P("ep", "tp", None, None),
            P("ep", "tp"),
            P("ep", "tp"),
            P("ep", "tp"),
            P("ep", "tp"),
            P("tp"),
            P(None, "tp"),
            P(),
            P(),
            P("ep", None, "tp"),
            P("ep", None, "tp"),
            P("ep", None, "tp"),
            P("ep", None),
            P("ep", None),
        ),
        out_specs=(P("ep", "tp"), P("ep", "tp", None, None)),
        check_vma=False,
    )
```

```python
import functools

import jax
import jax.numpy as jnp
import numpy as np
from jax import lax
from jax.experimental import pallas as pl
from jax.experimental.pallas import tpu as pltpu
from jax.sharding import PartitionSpec as P

MESH = pl.DeviceIdType.MESH
F32 = jnp.float32
BF16 = jnp.bfloat16
D = 4096
RD = 2048
HEADS = 16
HEAD = 128
ROWS = 40
COLS = 256
NEP = 16
NTP = 16
NZ = 8
SLOTS = 128
MESSAGES = 2
PER = NZ // MESSAGES
LIMIT = 67043328 - 40 * 128 * 128 * 4 - 2 * 16384 * 2
GROUPS_OF_ROWS = ROWS // 8
EPS = 1e-06


def constants():
    table = np.zeros((24, 128), np.float64)
    heads = np.arange(HEADS, dtype=np.float64)
    table[:HEADS] = (1.0 - 2.0 ** (-5.0 - 5.0 * heads / (HEADS - 1)))[:, None]
    inverse = 10000.0 ** (-np.arange(0, HEAD, 2, dtype=np.float64) / HEAD)
    table[HEADS] = np.concatenate([inverse, inverse])
    return table.astype(np.float32)


TRACE = False
_open = []


def mark(name):
    if not TRACE:
        return
    while _open:
        _open.pop().__exit__(None, None, None)
    if name:
        _open.append(jax.named_scope(name))
        _open[-1].__enter__()


def ring_offset(i):
    half = i // 2 + 1
    return half + ((i + 1) % 2) * (NZ - 2 * half)


def body(
    hidden,
    positions,
    ret_state,
    query_weight,
    key_weight,
    value_weight,
    gate_weight,
    head_gain,
    out_weight,
    mix_gain,
    ffn_gain,
    expert_gate,
    expert_up,
    expert_down,
    route_ids,
    route_weight,
    table,
    updated,
    v_state,
    v_hidden,
    v_pos,
    v_qkvg,
    v_head_gain,
    v_out,
    v_mix_gain,
    v_ffn_gain,
    v_gu,
    v_down,
    v_ids,
    v_weight,
    v_table,
    agbuf,
    xbuf,
    bacc,
    bsend,
    brecv,
    ssout,
    ssin,
    readbuf,
    spread,
    combine_terms,
    cbuf,
    afters,
    psend,
    dbuf,
    lifted,
    acc_gu,
    ebuf,
    acc_down,
    fsend,
    frecv,
    local_sem,
    gu_sem,
    w_send,
    w_recv,
    a1_send,
    a1_recv,
    a2_send,
    a2_recv,
    ss_sem,
    b_send,
    b_recv,
    c_send,
    c_fwd,
    c_recv,
    g_send,
    g_recv,
    d_send,
    d_fwd,
    d_recv,
    d_other,
    e_send,
    e_fwd,
    e_recv,
    f_send,
    f_recv,
):
    ep = lax.axis_index("ep")
    tp = lax.axis_index("tp")
    z = tp // 2
    core = tp % 2
    other = 2 * z + 1 - core
    down = ep // 4
    across = ep % 4

    mark("load")
    loads = [
        (hidden, v_hidden),
        (positions, v_pos),
        (table, v_table),
        (route_ids, v_ids),
        (route_weight, v_weight),
        (head_gain, v_head_gain),
        (mix_gain, v_mix_gain),
        (ffn_gain, v_ffn_gain),
        (query_weight, v_qkvg.at[across, :, pl.ds(0, 128)]),
        (key_weight, v_qkvg.at[across, :, pl.ds(128, 128)]),
        (value_weight, v_qkvg.at[across, :, pl.ds(256, 128)]),
        (gate_weight, v_qkvg.at[across, :, pl.ds(384, 128)]),
        (ret_state, v_state),
        (out_weight, v_out),
        (expert_down, v_down),
    ]
    copies = [pltpu.make_async_copy(src, dst, local_sem.at[i]) for i, (src, dst) in enumerate(loads)]
    for copy in copies[:12]:
        copy.start()

    def relative(i):
        return (z + (i + 1) // 2 * (1 - i % 2 * 2) + NZ) % NZ

    def lift_load(i, up):
        parity, place = i // NZ, i % NZ
        source = pl.multiple_of((2 * relative(place) + parity) * COLS, COLS)
        return pltpu.make_async_copy(
            (expert_up if up else expert_gate).at[:, pl.ds(source, COLS)],
            v_gu.at[:, pl.ds(pl.multiple_of(i * COLS, COLS), COLS), pl.ds(128 * up, 128)],
            gu_sem.at[i, up],
        )

    def lift_loads(i, carry):
        lift_load(i, 0).start()
        lift_load(i, 1).start()
        return carry

    def lift_loaded(i, carry):
        lift_load(i, 0).wait()
        lift_load(i, 1).wait()
        return carry

    barrier = pltpu.get_barrier_semaphore()

    def greet_plane(i, carry):
        peer = (ep + i) % NEP
        pl.semaphore_signal(barrier, inc=1, device_id=(peer, tp), device_id_type=MESH)
        pl.semaphore_signal(barrier, inc=1, device_id=(peer, other), device_id_type=MESH)
        return carry

    def greet_ring(i, carry):
        peer = 2 * ((z + i) % NZ) + core
        pl.semaphore_signal(barrier, inc=1, device_id=(ep, peer), device_id_type=MESH)
        return carry

    lax.fori_loop(1, NEP, greet_plane, 0)
    lax.fori_loop(1, NZ, greet_ring, 0)
    pl.semaphore_signal(barrier, inc=1, device_id=(ep, other), device_id_type=MESH)
    for copy in copies[12:]:
        copy.start()
    lax.fori_loop(0, NTP, lift_loads, 0)
    for copy in copies[:8]:
        copy.wait()
    agbuf[pl.ds(z, 1)] = v_hidden[...].reshape(1, ROWS, COLS)

    mark("prep")
    token = lax.broadcasted_iota(jnp.int32, (ROWS, ROWS), 0)
    other_token = lax.broadcasted_iota(jnp.int32, (ROWS, ROWS), 1)

    def column(row):
        return jnp.sum(jnp.where(token == other_token, row.astype(F32), 0.0), axis=1, keepdims=True)

    inverse = v_table[HEADS : HEADS + 1, :]
    angle = column(v_pos[...]) * inverse
    cosine = jnp.cos(angle)
    sine = jnp.sin(angle)
    lane = lax.broadcasted_iota(jnp.int32, (ROWS, 128), 1)
    sine = jnp.where(lane < HEAD // 2, -sine, sine)

    slot_expert = lane // 4
    slot_expert = slot_expert.astype(F32)
    first = column(v_ids[0:1, :]) == slot_expert
    second = column(v_ids[1:2, :]) == slot_expert
    named = jnp.where(first | second, 1.0, 0.0).astype(F32)
    earlier = jnp.where(token > other_token, 1.0, 0.0).astype(BF16)
    ranks = jnp.dot(earlier, named.astype(BF16), preferred_element_type=F32)
    placed = jnp.where(ranks == (lane % 4).astype(F32), named, 0.0)
    combine = placed * jnp.where(first, column(v_weight[0:1, :]), column(v_weight[1:2, :]))
    high = combine.astype(BF16).astype(F32)
    middle = (combine - high).astype(BF16).astype(F32)
    combine_terms[...] = jnp.concatenate(
        [high, middle, combine - high - middle, jnp.zeros((8, 128), F32)], axis=0
    ).astype(BF16)

    own_block = (
        lax.rem(lax.broadcasted_iota(jnp.int32, (32, 8 * HEAD), 0), 8)
        == lax.broadcasted_iota(jnp.int32, (32, 8 * HEAD), 1) // HEAD
    )
    spread[...] = jnp.where(own_block, 1.0, 0.0).astype(BF16)

    mark("barrier")
    pl.semaphore_wait(barrier, 2 * (NEP - 1) + (NZ - 1) + 1)

    def copy_to(src, dst, send_sem, recv_sem, to_ep, to_tp):
        return pltpu.make_async_remote_copy(
            src_ref=src,
            dst_ref=dst,
            send_sem=send_sem,
            recv_sem=recv_sem,
            device_id=(to_ep, to_tp),
            device_id_type=MESH,
        )

    right = 4 * down + (across + 1) % 4
    left = 4 * down + (across + 3) % 4

    def w_copy(block, half, way, i):
        part = v_qkvg.at[block, pl.ds(half * 128, 128)]
        return copy_to(
            part, part, w_send.at[way, i], w_recv.at[block, half], right if way == 0 else left, tp
        )

    for copy in copies[8:12]:
        copy.wait()
    w_sends = [
        w_copy(across, 0, 0, 0),
        w_copy(across, 1, 1, 0),
        w_copy(across, 1, 0, 1),
        w_copy(across, 0, 1, 1),
        w_copy(left % 4, 0, 0, 2),
        w_copy(right % 4, 1, 1, 2),
    ]

    def a1_copy(i, slot):
        peer = 2 * ((z + ring_offset(i)) % NZ) + core
        return copy_to(v_hidden, agbuf.at[slot], a1_send.at[i], a1_recv.at[slot], ep, peer)

    def a1_start(i, carry):
        a1_copy(NZ - 2 - i, z).start()
        return carry

    lax.fori_loop(0, NZ - 1, a1_start, 0)
    for copy in w_sends[:4]:
        copy.start()

    def near(i):
        return i + (i // 2) * (5 - 2 * i)

    def a2_copy(row, cc):
        return copy_to(
            agbuf.at[pl.ds(2 * row, 2)],
            xbuf.at[down, core],
            a2_send.at[row, cc],
            a2_recv.at[down, core],
            4 * row + across,
            2 * z + cc,
        )

    def a2_start(i, carry):
        row = (z // 2 + near(i)) % 4
        for k in range(2):
            slot = 2 * row + k

            @pl.when(slot != z)
            def _():
                a1_copy(0, slot).wait_recv()

        for cc in range(2):
            mine = (row == down) & (cc == core)

            @pl.when(jnp.logical_not(mine))
            def _():
                a2_copy(row, cc).start()

            @pl.when(mine)
            def _():
                xbuf[pl.ds(row, 1), pl.ds(core, 1)] = agbuf[pl.ds(2 * row, 2)].reshape(
                    1, 1, 2, ROWS, COLS
                )

        return carry

    mark("a1_wait_a2_issue")
    lax.fori_loop(0, 4, a2_start, 0)
    mark("w_forward")
    w_copy(left % 4, 0, 0, 0).wait_recv()
    w_sends[4].start()
    w_copy(right % 4, 1, 1, 0).wait_recv()
    w_sends[5].start()

    mark("ss")
    def square(i, total):
        part = agbuf[pl.ds(i, 1)].reshape(ROWS, COLS).astype(F32)
        part = part * part
        return total + part[:, :128] + part[:, 128:]

    ssout[...] = lax.fori_loop(0, NZ, square, jnp.zeros((ROWS, 128), F32))
    ss_copy = copy_to(ssout, ssin, ss_sem.at[0], ss_sem.at[1], ep, other)
    ss_copy.start()

    steps = (0, 1, 3, 2)
    plane = [
        4 * lax.rem(down + row, 4) + lax.rem(across + column_step, 4)
        for row, column_step in sorted(
            ((row, column_step) for row in range(4) for column_step in range(4)),
            key=lambda step: min(step[0], 4 - step[0]) + min(step[1], 4 - step[1]),
        )
    ]

    def b_copy(slot, row):
        return copy_to(
            bsend.at[row], brecv.at[slot], b_send.at[row], b_recv.at[slot], 4 * row + across, tp
        )

    mark("a2_wait")
    for row in range(4):
        for parity in range(2):

            @pl.when((row != down) | (parity != core))
            def _():
                block = xbuf.at[row, parity]
                copy_to(block, block, a2_send.at[0, 0], a2_recv.at[row, parity], ep, other).wait_recv()

    def partial(block):
        at = pl.multiple_of((4 * down + block) * COLS, COLS)
        gain = v_mix_gain[:, pl.ds(at, COLS)].reshape(1, 1, COLS)
        rows = xbuf[:, pl.ds(block % 2, 1), pl.ds(block // 2, 1)].reshape(4, ROWS, COLS)
        rows = (rows.astype(F32) * gain).reshape(4 * ROWS, COLS).astype(BF16)
        return jnp.dot(
            rows, v_qkvg[pl.ds(block, 1)].reshape(COLS, 512), preferred_element_type=F32
        )

    mark("b_rows")
    bacc[...] = partial(across)
    w_copy(left % 4, 1, 0, 0).wait_recv()
    bacc[...] += partial(left % 4)
    w_copy(right % 4, 0, 1, 0).wait_recv()
    bacc[...] += partial(right % 4)
    opposite = (across + 2) % 4
    mark("w_wait")
    w_copy(opposite, 0, 0, 0).wait_recv()
    w_copy(opposite, 1, 1, 0).wait_recv()
    mark("b_last")
    bsend[...] = (bacc[...] + partial(opposite)).reshape(4, ROWS, 512).astype(BF16)

    def b_start(i, carry):
        b_copy(down, (down + near(3 - i)) % 4).start()
        return carry

    lax.fori_loop(0, 3, b_start, 0)
    brecv[pl.ds(down, 1)] = bsend[pl.ds(down, 1)]

    mark("ss_wait")
    ss_copy.wait_recv()
    square_sum = jnp.sum(ssout[...] + ssin[...], axis=-1, keepdims=True)
    factor = lax.rsqrt(square_sum * (1.0 / D) + EPS)

    mark("b_sum")

    def b_wait(i, carry):
        row = (down + near(i)) % 4
        b_copy(row, row).wait_recv()
        return carry

    lax.fori_loop(1, 4, b_wait, 0)
    part = brecv[...].astype(F32)
    joined = (part[0] + part[1]) + (part[2] + part[3])
    joined = (joined * factor).astype(BF16).astype(F32)

    mark("rot")
    def rotate(values):
        return values * cosine + pltpu.roll(values, HEAD // 2, 1) * sine

    rotated_query = rotate(joined[:, :128])
    rotated_key = rotate(joined[:, 128:256]) * HEAD ** (-0.5)
    value = joined[:, 256:384]
    gate_rows = joined[:, 384:]
    decay = v_table[pl.ds(tp, 1), :]
    readbuf[0] = rotated_query
    readbuf[1] = rotated_key
    readbuf[2] = value
    mark("retain")
    copies[12].wait()

    def terms(rows):
        high = rows.astype(BF16).astype(F32)
        middle = (rows - high).astype(BF16).astype(F32)
        low = rows - high - middle
        return jnp.concatenate([high, middle, low, jnp.zeros_like(rows)], axis=0).astype(BF16)

    def over_rows(stack, columns):
        return lax.dot_general(
            stack, columns, (((0,), (0,)), ((), ())), preferred_element_type=F32
        )

    def retain(group, carry):
        at = pl.ds(pl.multiple_of(8 * group, 8), 8)
        values = jnp.concatenate([readbuf[2, at, :]] * 4, axis=0)
        values = jnp.where(own_block, jnp.concatenate([values] * 8, axis=1), 0.0).astype(BF16)
        outer = over_rows(terms(readbuf[1, at, :]), values)
        query = over_rows(terms(readbuf[0, at, :]), spread[...])
        reads = []
        for k in range(8):
            block = slice(k * HEAD, (k + 1) * HEAD)
            state = decay * v_state[8 * group + k, 0] + outer[:, block]
            v_state[8 * group + k, 0] = state
            reads.append(jnp.sum(query[:, block] * state, axis=0, keepdims=True))
        readbuf[3, at, :] = jnp.concatenate(reads, axis=0)
        return carry

    for group in range(ROWS // 8):
        retain(group, 0)
    mark("groupnorm")
    read = readbuf[3]
    centered = read - jnp.mean(read, axis=-1, keepdims=True)
    normal = centered * lax.rsqrt(jnp.mean(centered * centered, axis=-1, keepdims=True) + EPS)
    mixed = normal * v_head_gain[...] * jax.nn.silu(gate_rows)
    cbuf[pl.ds(tp, 1)] = mixed.astype(BF16).reshape(1, ROWS, HEAD)

    def gather(buf, send_sem, fwd_sem, recv_sem, consume, both=False, lag=0):
        def direct(i, slot):
            peer = 2 * ((z + ring_offset(i)) % NZ) + core
            return copy_to(buf.at[slot], buf.at[slot], send_sem.at[i], recv_sem.at[slot], ep, peer)

        def forward(row, slot):
            return copy_to(
                buf.at[slot], buf.at[slot], fwd_sem.at[row], recv_sem.at[slot], ep, other
            )

        def cross(i, slot):
            peer = 2 * lax.rem(z + ring_offset(i), NZ) + 1 - core
            return copy_to(
                buf.at[slot], buf.at[slot], fwd_sem.at[i], recv_sem.at[slot], ep, peer
            )

        def begin(i, carry):
            direct(i, tp).start()
            if both:
                cross(i, tp).start()
            return carry

        lax.fori_loop(0, NZ - 1, begin, 0)
        forward(NZ - 1 if both else z, tp).start()

        def step(i, carry):
            @pl.when(i < NZ - 1)
            def _():
                row = (z + ring_offset(i)) % NZ
                direct(0, 2 * row + core).wait_recv()
                if not both:
                    forward(row, 2 * row + core).start()

            @pl.when(i >= lag)
            def _():
                place = i - lag
                before = relative(place)
                forward(before, 2 * before + 1 - core).wait_recv()
                consume(before, place == 0)

            return carry

        lax.fori_loop(0, NZ + lag, step, 0)

        def finish():
            def one(i, carry):
                direct(i, tp).wait_send()
                forward(i if both else (z + ring_offset(i)) % NZ, tp).wait_send()
                return carry

            lax.fori_loop(0, NZ - 1, one, 0)
            forward(NZ - 1 if both else z, tp).wait_send()

        return finish

    copies[13].wait()
    projected = readbuf.at[pl.ds(0, 2)]

    def project(row, first_step):
        pair = cbuf[pl.ds(2 * row, 2)].astype(F32)
        block = jnp.concatenate([pair[0], pair[1]], axis=1).astype(BF16)
        part = jnp.dot(
            block,
            v_out[pl.ds(pl.multiple_of(row * COLS, COLS), COLS), :],
            preferred_element_type=F32,
        )

        @pl.when(first_step)
        def _():
            projected[0] = part[:, :128]
            projected[1] = part[:, 128:]

        @pl.when(jnp.logical_not(first_step))
        def _():
            projected[0] += part[:, :128]
            projected[1] += part[:, 128:]

    mark("c_gather")
    finish_c = gather(cbuf, c_send, c_fwd, c_recv, project, lag=1)
    mark("after_pack")
    own = v_hidden[...].astype(F32)
    after = (own + jnp.concatenate([projected[0], projected[1]], axis=1)).astype(BF16)
    afters[pl.ds(z, 1)] = after.reshape(1, ROWS, COLS)

    def g_copy(i, slot):
        peer = 2 * ((z + ring_offset(i)) % NZ) + core
        return copy_to(afters.at[z], afters.at[slot], g_send.at[i], g_recv.at[slot], ep, peer)

    def g_start(i, carry):
        g_copy(i, z).start()
        return carry

    lax.fori_loop(0, NZ - 1, g_start, 0)

    def halves_below(array):
        parts = [array[:, :128].reshape(NEP, 8, 128), array[:, 128:].reshape(NEP, 8, 128)]
        return jnp.concatenate(parts, axis=1)

    def halves_beside(array):
        array = array.astype(F32)
        return array[:, :8].reshape(SLOTS, 128), array[:, 8:].reshape(SLOTS, 128)

    placing = placed.astype(BF16)

    def pack(half, k):
        packed = lax.dot_general(
            placing,
            afters[pl.ds(relative(PER * half + k), 1)].reshape(ROWS, COLS),
            (((0,), (0,)), ((), ())),
            preferred_element_type=F32,
        )
        packed = halves_below(packed).astype(BF16)
        psend[half, :, pl.ds(k, 1)] = packed.reshape(NEP, 1, 16, 128)

    def d_copy(half, peer, source):
        return copy_to(
            psend.at[half, peer],
            dbuf.at[core, half, source],
            d_send.at[half, peer],
            d_recv.at[half, source],
            peer,
            tp,
        )

    def d_forward(half, parity, source):
        block = dbuf.at[parity, half, source]
        return copy_to(block, block, d_fwd.at[half, source], d_other.at[half, source], ep, other)

    def pack_next(half):
        def one(k, carry):
            g_copy(PER * half + k - 1, relative(PER * half + k)).wait_recv()
            pack(half, k)
            return carry

        return one

    pack(0, 0)
    acc_gu[...] = jnp.zeros_like(acc_gu)
    for half in range(MESSAGES):
        mark(f"after_gather{half}")
        lax.fori_loop(0 if half else 1, PER, pack_next(half), 0)
        mark(f"d_issue{half}")
        for peer in plane[:0:-1]:
            d_copy(half, peer, ep).start()
        dbuf[pl.ds(core, 1), half, pl.ds(ep, 1)] = psend[half, pl.ds(ep, 1)].reshape(
            1, 1, PER, 16, 128
        )
        d_forward(half, core, ep).start()

    def d_arrive(half):
        for peer in plane[1:]:
            d_copy(half, peer, peer).wait_recv()
            d_forward(half, core, peer).start()

    def d_other_wait(half):
        def one(source, carry):
            d_forward(half, 1 - core, source).wait_recv()
            return carry

        return one

    square_of = acc_gu.at[2]

    def lift(half, parity):
        for k in range(PER):
            at = pl.multiple_of((2 * relative(PER * half + k) + parity) * COLS, COLS)
            block = dbuf[pl.ds(parity, 1), half, :, k].reshape(NEP, 16, 128)
            low, high = halves_beside(block)
            square_of[:, :128] += low * low + high * high
            both = jnp.concatenate([low, high], axis=1) * v_ffn_gain[:, pl.ds(at, COLS)]
            lifted[:, k * COLS : (k + 1) * COLS] = both.astype(BF16)
        at = pl.multiple_of((parity * NZ + PER * half) * COLS, PER * COLS)
        for j in range(2):
            acc_gu[j] += jnp.dot(
                lifted[...], v_gu[j, pl.ds(at, PER * COLS), :], preferred_element_type=F32
            )

    for half in range(MESSAGES):
        mark(f"d_wait{half}")
        d_arrive(half)
        if half == 0:
            lax.fori_loop(0, NTP, lift_loaded, 0)
        else:
            lax.fori_loop(0, NEP, d_other_wait(half - 1), 0)
            mark(f"lift_other{half - 1}")
            lift(half - 1, 1 - core)
        mark(f"lift_own{half}")
        lift(half, core)
    mark("lift_wait")
    lax.fori_loop(0, NEP, d_other_wait(MESSAGES - 1), 0)
    mark("lift_last")
    lift(MESSAGES - 1, 1 - core)
    mark("act")
    inner = lax.rsqrt(
        jnp.sum(square_of[:, :128], axis=-1, keepdims=True) * (1.0 / D) + EPS
    )
    own_expert = lax.broadcasted_iota(jnp.int32, (SLOTS, COLS), 0) % 8 < 4
    chosen = jnp.where(own_expert, acc_gu[0], acc_gu[1]) * inner
    activated = jax.nn.silu(chosen[:, :128]) * chosen[:, 128:]
    ebuf[pl.ds(tp, 1)] = activated.astype(BF16).reshape(1, SLOTS, 128)
    copies[14].wait()

    def lower(row, first_step):
        @pl.when(first_step)
        def _():
            acc_down[...] = jnp.zeros_like(acc_down)

        pair = ebuf[pl.ds(2 * row, 2)]
        both = jnp.concatenate([pair[0], pair[1]], axis=1)
        at = pl.multiple_of(row * COLS, COLS)
        for j in range(2):
            acc_down[j] += jnp.dot(both, v_down[j, pl.ds(at, COLS), :], preferred_element_type=F32)

    mark("e_gather")
    finish_e = gather(ebuf, e_send, e_fwd, e_recv, lower, lag=1)
    mark("result")
    result = jnp.where(own_expert, acc_down[0], acc_down[1])

    fsend[...] = halves_below(result).astype(BF16)

    def f_copy(peer, source):
        return copy_to(
            fsend.at[peer], frecv.at[source], f_send.at[peer], f_recv.at[source], peer, tp
        )

    for peer in plane[:0:-1]:
        f_copy(peer, ep).start()
    frecv[pl.ds(ep, 1)] = fsend[pl.ds(ep, 1)]

    mark("sent")
    def sent_ring(i, carry):
        a1_copy(i, z).wait_send()
        g_copy(i, z).wait_send()
        return carry

    lax.fori_loop(0, NZ - 1, sent_ring, 0)

    for row in range(4):
        for cc in range(2):

            @pl.when((row != down) | (cc != core))
            def _():
                a2_copy(row, cc).wait_send()

    for copy in w_sends:
        copy.wait_send()

    def sent_b(i, carry):
        b_copy(down, (down + near(i)) % 4).wait_send()
        return carry

    lax.fori_loop(1, 4, sent_b, 0)
    ss_copy.wait_send()
    for half in range(MESSAGES):
        d_forward(half, core, ep).wait_send()

    def sent_plane(i, carry):
        peer = (ep + i) % NEP
        for half in range(MESSAGES):
            d_copy(half, peer, ep).wait_send()
            d_forward(half, core, peer).wait_send()
        return carry

    lax.fori_loop(1, NEP, sent_plane, 0)
    finish_c()
    finish_e()

    def f_wait(i, carry):
        peer = (ep + i) % NEP
        f_copy(peer, peer).wait_recv()
        return carry

    mark("f_wait")
    lax.fori_loop(1, NEP, f_wait, 0)
    mark("combine")
    back = jnp.concatenate(halves_beside(frecv[...]), axis=1)
    weighted = jnp.dot(combine_terms[...], back.astype(BF16), preferred_element_type=F32)
    weighted = weighted[:ROWS] + weighted[ROWS : 2 * ROWS] + weighted[2 * ROWS : 3 * ROWS]
    updated[...] = (after.astype(F32) + weighted).astype(BF16)

    def f_sent(i, carry):
        f_copy((ep + i) % NEP, ep).wait_send()
        return carry

    lax.fori_loop(1, NEP, f_sent, 0)
    mark("")


def state_body(before, state, updated, next_state, sem):
    copies = [
        pltpu.make_async_copy(before, updated, sem.at[0]),
        pltpu.make_async_copy(state, next_state, sem.at[1]),
    ]
    for copy in copies:
        copy.start()
    for copy in copies:
        copy.wait()


def per_device(
    hidden,
    positions,
    ret_state,
    query_weight,
    key_weight,
    value_weight,
    gate_weight,
    head_gain,
    out_weight,
    mix_gain,
    ffn_gain,
    expert_gate,
    expert_up,
    expert_down,
    route_ids,
    route_weight,
):
    table = jnp.asarray(constants())
    dma = pltpu.SemaphoreType.DMA
    vmem = pltpu.VMEM
    anywhere = pl.BlockSpec(memory_space=pltpu.HBM)
    updated, parts = pl.pallas_call(
        body,
        out_shape=(
            pltpu.VMEM((ROWS, COLS), BF16),
            pltpu.VMEM(ret_state.shape, F32),
        ),
        in_specs=[anywhere] * 17,
        out_specs=(pl.BlockSpec(memory_space=pltpu.VMEM),) * 2,
        scratch_shapes=[
            vmem((ROWS, COLS), BF16),
            vmem((1, ROWS), jnp.int32),
            vmem((4, COLS, 512), BF16),
            vmem((1, HEAD), F32),
            vmem((RD, COLS), BF16),
            vmem((1, D), F32),
            vmem((1, D), F32),
            vmem((2, D, COLS), BF16),
            vmem((2, RD, COLS), BF16),
            vmem((2, ROWS), jnp.int32),
            vmem((2, ROWS), F32),
            vmem((24, 128), F32),
            vmem((NZ, ROWS, COLS), BF16),
            vmem((4, 2, 2, ROWS, COLS), BF16),
            vmem((4 * ROWS, 512), F32),
            vmem((4, ROWS, 512), BF16),
            vmem((4, ROWS, 512), BF16),
            vmem((ROWS, 128), F32),
            vmem((ROWS, 128), F32),
            vmem((4, ROWS, HEAD), F32),
            vmem((32, 8 * HEAD), BF16),
            vmem((128, 128), BF16),
            vmem((NTP, ROWS, HEAD), BF16),
            vmem((NZ, ROWS, COLS), BF16),
            vmem((MESSAGES, NEP, PER, 16, 128), BF16),
            vmem((2, MESSAGES, NEP, PER, 16, 128), BF16),
            vmem((SLOTS, PER * COLS), BF16),
            vmem((3, SLOTS, COLS), F32),
            vmem((NTP, SLOTS, 128), BF16),
            vmem((2, SLOTS, COLS), F32),
            vmem((NEP, 16, 128), BF16),
            vmem((NEP, 16, 128), BF16),
            dma((15,)),
            dma((NTP, 2)),
            dma((2, 3)),
            dma((4, 2)),
            dma((NZ,)),
            dma((NZ,)),
            dma((4, 2)),
            dma((4, 2)),
            dma((2,)),
            dma((4,)),
            dma((4,)),
            dma((NZ,)),
            dma((NZ,)),
            dma((NTP,)),
            dma((NZ,)),
            dma((NZ,)),
            dma((MESSAGES, NEP)),
            dma((MESSAGES, NEP)),
            dma((MESSAGES, NEP)),
            dma((MESSAGES, NEP)),
            dma((NZ,)),
            dma((NZ,)),
            dma((NTP,)),
            dma((NEP,)),
            dma((NEP,)),
        ],
        compiler_params=pltpu.CompilerParams(
            collective_id=0, has_side_effects=True, vmem_limit_bytes=LIMIT
        ),
    )(
        hidden,
        positions.reshape(1, ROWS),
        ret_state,
        query_weight,
        key_weight,
        value_weight,
        gate_weight,
        head_gain.reshape(1, HEAD),
        out_weight,
        mix_gain.reshape(1, D),
        ffn_gain.reshape(1, D),
        expert_gate,
        expert_up,
        expert_down,
        route_ids.T,
        route_weight.T,
        table,
    )
    return pl.pallas_call(
        state_body,
        out_shape=(
            jax.ShapeDtypeStruct((ROWS, COLS), BF16),
            jax.ShapeDtypeStruct(ret_state.shape, F32),
        ),
        in_specs=[pl.BlockSpec(memory_space=pl.ANY)] * 2,
        out_specs=(anywhere,) * 2,
        scratch_shapes=[dma((2,))],
        compiler_params=pltpu.CompilerParams(vmem_limit_bytes=1024 * 1024),
    )(updated, parts)


def solution(mesh):
    return jax.shard_map(
        per_device,
        mesh=mesh,
        in_specs=(
            P("ep", "tp"),
            P("ep"),
            P("ep", "tp", None, None),
            P("ep", "tp"),
            P("ep", "tp"),
            P("ep", "tp"),
            P("ep", "tp"),
            P("tp"),
            P(None, "tp"),
            P(),
            P(),
            P("ep", None, "tp"),
            P("ep", None, "tp"),
            P("ep", None, "tp"),
            P("ep", None),
            P("ep", None),
        ),
        out_specs=(P("ep", "tp"), P("ep", "tp", None, None)),
        check_vma=False,
    )
```
